512 devices in a mesh: sp: 64 (over z, y), tp: 8 (over x, core).
Axes of the slice: x: 4, y: 4, z: 16, core: 2. Of those that a mesh axis runs over, the one named last changes fastest.
Arguments:
- tokens: bfloat16 [16384, 2048], P(('sp', 'tp')), may hold values from -6 to 6
- norm_gain: float32 [2048], replicated, may hold values from 0.1 to 1.9
- recept_weight: bfloat16 [2048, 1024], P(None, 'tp'), may hold values from -0.125 to 0.125
- key_weight: bfloat16 [2048, 1024], P(None, 'tp'), may hold values from -0.125 to 0.125
- value_weight: bfloat16 [2048, 1024], P(None, 'tp'), may hold values from -0.125 to 0.125
- decay_down_weight: bfloat16 [2048, 64], replicated, may hold values from -0.125 to 0.125
- rate_down: bfloat16 [2048, 64], replicated, may hold values from -0.125 to 0.125
- decay_up: bfloat16 [64, 1024], P(None, 'tp'), may hold values from -0.75 to 0.75
- rate_up: bfloat16 [64, 1024], P(None, 'tp'), may hold values from -0.75 to 0.75
- decay_base: float32 [1024], P('tp'), may hold values from -16 to -3
- rate_base: float32 [1024], P('tp'), may hold values from -12 to 1
- decay_extra: float32 [16384, 16], P('sp', 'tp'), may hold values from -3 to 0
- group_gain: float32 [1024], P('tp'), may hold values from 0.1 to 1.9
- attn_query: bfloat16 [2048, 1024], P(None, 'tp'), may hold values from -0.125 to 0.125
- attn_key: bfloat16 [2048, 1024], P(None, 'tp'), may hold values from -0.125 to 0.125
- attn_value: bfloat16 [2048, 1024], P(None, 'tp'), may hold values from -0.125 to 0.125
- query_gain: float32 [64], replicated, may hold values from 1 to 9
- key_gain: float32 [64], replicated, may hold values from 1 to 9
- lambdas: float32 [8], P('tp'), may hold values from 0.3 to 0.8
- head_gain: float32 [128], replicated, may hold values from 0.1 to 1.9
- out_linear: bfloat16 [1024, 2048], P('tp'), may hold values from -0.15625 to 0.15625
- out_attn: bfloat16 [1024, 2048], P('tp'), may hold values from -0.1875 to 0.1875
Outputs:
- mixed: bfloat16 [16384, 2048], P(('sp', 'tp'))
The draws below stay inside these ranges and needn't reach their ends.
All inputs are finite; a program needn't handle non-finite values.
Results may differ from the reference program's by a relative error of at most 0.018.
The reference program's roundings to bfloat16 on the way (of `normed`, `linear_part`, `weights` and `attn_part`) count: a program that leaves them out, or rounds other values in their place, can miss the bound.
Values may be sent and summed in bfloat16 or wider, within the bound.
No kernel may reach another device: no remote copies, remote signals or barrier semaphores. Data moves between devices by JAX's collectives and lax.ppermute only.
A program may use at most 128 MiB of HBM per device.

```python
import math
import jax
import jax.numpy as jnp
from jax import lax

D = 2048
LINEAR_HEAD_WIDTH = 64
HEADS_A = 16
HEAD_C = 64
HEADS_C = 8
LOW = 64
TOK_DEV = 256
TOKENS = 16384


def rate_tables(key):
    base_key = jax.random.fold_in(key, 11)
    width = HEADS_A * LINEAR_HEAD_WIDTH
    ordering = jax.random.permutation(jax.random.fold_in(base_key, 1), HEADS_A)
    fast_heads = ordering < HEADS_A // 2
    fast_chan = jnp.repeat(fast_heads, LINEAR_HEAD_WIDTH)
    spread_one = jax.random.uniform(jax.random.fold_in(base_key, 2), (width,), jnp.float32)
    spread_two = jax.random.uniform(jax.random.fold_in(base_key, 3), (width,), jnp.float32)
    fast_decay = math.log(1.0 / 50.0) + spread_one * math.log(50.0 / 30.0)
    slow_decay = jnp.log(0.1 / TOKENS) + spread_one - 0.5
    fast_rate = 2.0 * spread_two - 1.0
    slow_rate = jnp.log(16.0 / TOKENS) + spread_two - 0.5
    return (jnp.where(fast_chan, fast_decay, slow_decay), jnp.where(fast_chan, fast_rate, slow_rate))


def draw_decay_base(key, part):
    return rate_tables(key)[0].astype(jnp.float32)


def draw_rate_base(key, part):
    return rate_tables(key)[1].astype(jnp.float32)


def draw_decay_extra(key, part):
    base_key = jax.random.fold_in(key, 23)
    blocks = TOKENS // TOK_DEV
    block_rates = jnp.exp(jax.random.uniform(jax.random.fold_in(base_key, 1), (blocks, HEADS_A), jnp.float32, math.log(0.25), 0.0)) / TOKENS
    steady = -jnp.repeat(block_rates, TOK_DEV, axis=0)
    spots = jax.random.randint(jax.random.fold_in(base_key, 2), (3,), 0, TOKENS)
    losses = jax.random.uniform(jax.random.fold_in(base_key, 3), (3, HEADS_A), jnp.float32, 0.2, 0.5)
    hits = (jnp.arange(TOKENS)[:, None] == spots[None, :]).astype(jnp.float32)
    return (steady + jnp.dot(hits, jnp.log(1.0 - losses))).astype(jnp.float32)


def gain_tables(key):
    base_key = jax.random.fold_in(key, 37)
    gain_query = jax.random.uniform(jax.random.fold_in(base_key, 1), (HEAD_C,), jnp.float32, 1.15, 1.55)
    gain_key = jax.random.uniform(jax.random.fold_in(base_key, 2), (HEAD_C,), jnp.float32, 1.15, 1.55)
    return (gain_query, gain_key)


def draw_query_gain(key, part):
    return gain_tables(key)[0]


def draw_key_gain(key, part):
    return gain_tables(key)[1]


def shard_levels(own_key, shape, shards, smallest, high):
    level = 1.0
    for dim, parts in shards:
        draws = jax.random.uniform(jax.random.fold_in(jax.random.fold_in(own_key, 6), dim), (parts,), jnp.float32, smallest / len(shards), high / len(shards))
        level = level * jnp.repeat(jnp.exp(draws), shape[dim] // parts).reshape((-1,) + (1,) * (len(shape) - 1 - dim))
    return level


def bell_draw(own_key, dims, spread, most, cuts=(), kind=jnp.bfloat16):
    array = jax.random.normal(own_key, dims, jnp.float32) * spread
    if len(cuts) > 0:
        array = shard_levels(own_key, dims, cuts, -0.22, 0.18) * array
    return jnp.clip(array, min=-most, max=most).astype(kind)


def setup_inputs(seed: int = 0) -> dict:
    streams_of = jax.random.split(jax.random.key(seed), 23)
    return {
        "tokens": bell_draw(streams_of[0], (TOKENS, D), 1.0, 6.0, ((0, 512),)),
        "norm_gain": jnp.clip(1.0 + 0.18 * jax.random.normal(streams_of[1], (D,), jnp.float32), 0.1, 1.9),
        "recept_weight": bell_draw(streams_of[2], (D, HEADS_A * LINEAR_HEAD_WIDTH), D ** -0.5, 0.125, ((1, 8),)),
        "key_weight": bell_draw(streams_of[3], (D, HEADS_A * LINEAR_HEAD_WIDTH), D ** -0.5, 0.125, ((1, 8),)),
        "value_weight": bell_draw(streams_of[4], (D, HEADS_A * LINEAR_HEAD_WIDTH), D ** -0.5, 0.125, ((1, 8),)),
        "decay_down_weight": bell_draw(streams_of[5], (D, LOW), D ** -0.5, 0.125),
        "rate_down": bell_draw(streams_of[6], (D, LOW), D ** -0.5, 0.125),
        "decay_up": bell_draw(streams_of[7], (LOW, HEADS_A * LINEAR_HEAD_WIDTH), LOW ** -0.5, 0.75, ((1, 8),)),
        "rate_up": bell_draw(streams_of[8], (LOW, HEADS_A * LINEAR_HEAD_WIDTH), LOW ** -0.5, 0.75, ((1, 8),)),
        "decay_base": draw_decay_base(jax.random.fold_in(streams_of[22], 71), 0),
        "rate_base": draw_rate_base(jax.random.fold_in(streams_of[22], 71), 0),
        "decay_extra": draw_decay_extra(jax.random.fold_in(streams_of[22], 71), 0),
        "group_gain": jnp.clip(1.0 + 0.18 * jax.random.normal(streams_of[12], (HEADS_A * LINEAR_HEAD_WIDTH,), jnp.float32), 0.1, 1.9),
        "attn_query": bell_draw(streams_of[13], (D, HEADS_C * 2 * HEAD_C), D ** -0.5, 0.125, ((1, 8),)),
        "attn_key": bell_draw(streams_of[14], (D, HEADS_C * 2 * HEAD_C), D ** -0.5, 0.125, ((1, 8),)),
        "attn_value": bell_draw(streams_of[15], (D, HEADS_C * 2 * HEAD_C), D ** -0.5, 0.125, ((1, 8),)),
        "query_gain": draw_query_gain(jax.random.fold_in(streams_of[22], 71), 0),
        "key_gain": draw_key_gain(jax.random.fold_in(streams_of[22], 71), 0),
        "lambdas": jnp.clip(0.3 + 0.5 * jax.random.uniform(streams_of[18], (HEADS_C,), jnp.float32) ** shard_levels(streams_of[18], (HEADS_C,), ((0, 8),), -0.2, 0.2), 0.3, 0.8),
        "head_gain": jnp.clip(1.0 + 0.18 * jax.random.normal(streams_of[19], (2 * HEAD_C,), jnp.float32), 0.1, 1.9),
        "out_linear": bell_draw(streams_of[20], (HEADS_A * LINEAR_HEAD_WIDTH, D), (3 * HEADS_A * LINEAR_HEAD_WIDTH // 2) ** -0.5, 0.15625, ((0, 8),)),
        "out_attn": bell_draw(streams_of[21], (HEADS_C * 2 * HEAD_C, D), (HEADS_C * 2 * HEAD_C) ** -0.5, 0.1875, ((0, 8),)),
    }


precise_mode = lax.Precision.HIGHEST

def rms_scale(values, gain):
    return values * lax.rsqrt(lax.optimization_barrier(jnp.mean(values * values, -1, keepdims=True)) + 1e-06) * gain

def reference(tokens, norm_gain, recept_weight, key_weight, value_weight, decay_down_weight, rate_down, decay_up, rate_up, decay_base, rate_base, decay_extra, group_gain, attn_query, attn_key, attn_value, query_gain, key_gain, lambdas, head_gain, out_linear, out_attn):
    length = tokens.shape[0]
    normed = rms_scale(tokens.astype(jnp.float32), norm_gain).astype(jnp.bfloat16)

    def project(weight):
        return jnp.dot(normed, weight, preferred_element_type=jnp.float32).astype(jnp.bfloat16)

    def heads_a(values):
        return values.astype(jnp.float32).reshape(length, HEADS_A, LINEAR_HEAD_WIDTH)
    recept = heads_a(project(recept_weight))
    lin_key = heads_a(project(key_weight))
    lin_value = heads_a(project(value_weight))
    decay_low = project(decay_down_weight)
    rate_low = project(rate_down)
    decay_mix = jnp.dot(decay_low, decay_up, preferred_element_type=jnp.float32)
    rate_mix = jnp.dot(rate_low, rate_up, preferred_element_type=jnp.float32)
    log_decay = heads_a(-jnp.exp(decay_base[None, :] + jnp.tanh(decay_mix))) + decay_extra[:, :, None]
    rate_gate = heads_a(jax.nn.sigmoid(rate_base[None, :] + jnp.tanh(rate_mix)))
    unit_key = lin_key * lax.rsqrt(lax.optimization_barrier(jnp.sum(lin_key * lin_key, -1, keepdims=True)) + 1e-06)
    remove = -unit_key
    restore = unit_key * rate_gate
    inject = lin_key * rate_gate

    def token_step(memory, inputs):
        recept_t, decay_per_token, remove_t, restore_t, value_t, inject_t = inputs
        along = jnp.einsum('hij,hj->hi', memory, remove_t, precision=precise_mode)
        memory = memory * decay_per_token[:, None, :] + along[:, :, None] * restore_t[:, None, :] + value_t[:, :, None] * inject_t[:, None, :]
        return (memory, jnp.einsum('hij,hj->hi', memory, recept_t, precision=precise_mode))
    start_state = jnp.zeros((HEADS_A, LINEAR_HEAD_WIDTH, LINEAR_HEAD_WIDTH), jnp.float32)
    unused, read_out = lax.scan(token_step, start_state, (recept, jnp.exp(log_decay), remove, restore, lin_value, inject))
    head_mean = lax.optimization_barrier(jnp.mean(read_out, -1, keepdims=True))
    centered = read_out - head_mean
    head_var = lax.optimization_barrier(jnp.mean(centered * centered, -1, keepdims=True))
    linear_part = centered * lax.rsqrt(head_var + 0.00064) * group_gain.reshape(HEADS_A, LINEAR_HEAD_WIDTH)
    linear_part = linear_part.reshape(length, HEADS_A * LINEAR_HEAD_WIDTH).astype(jnp.bfloat16)
    raw_query = project(attn_query).astype(jnp.float32).reshape(length, HEADS_C, 2, HEAD_C)
    raw_key = project(attn_key).astype(jnp.float32).reshape(length, HEADS_C, 2, HEAD_C)
    values_c = project(attn_value).reshape(length, HEADS_C, 2 * HEAD_C)
    queries = rms_scale(raw_query, query_gain).astype(jnp.bfloat16)
    keys_normed = rms_scale(raw_key, key_gain).astype(jnp.bfloat16)
    score_scale = HEAD_C ** (-0.5)
    query_block = min(1024, length)
    pieces = []
    for first in range(0, length, query_block):
        finish = first + query_block
        query_pos = first + jnp.arange(query_block)
        key_pos = jnp.arange(finish)
        allowed = key_pos[None, :] <= query_pos[:, None]

        def one_head(operands):
            head_query, head_key, head_value, head_lambda = operands
            scores = jnp.einsum('qmd,kmd->mqk', head_query.astype(jnp.float32), head_key.astype(jnp.float32), precision=precise_mode) * score_scale
            scores = jnp.where(allowed[None], scores, -jnp.inf)
            row_top = lax.optimization_barrier(jnp.max(scores, -1, keepdims=True))
            expo = jnp.exp(scores - row_top)
            probability = expo / lax.optimization_barrier(jnp.sum(expo, -1, keepdims=True))
            weights = (probability[0] - head_lambda * probability[1]).astype(jnp.bfloat16)
            return jnp.dot(weights, head_value, preferred_element_type=jnp.float32)
        head_out = lax.map(one_head, (jnp.moveaxis(queries[first:finish], 1, 0), jnp.moveaxis(keys_normed[:finish], 1, 0), jnp.moveaxis(values_c[:finish], 1, 0), lambdas))
        pieces.append(jnp.moveaxis(head_out, 0, 1))
    attended = jnp.concatenate(pieces, axis=0)
    attn_part = rms_scale(attended, head_gain).astype(jnp.bfloat16).reshape(length, HEADS_C * 2 * HEAD_C)
    summed = jnp.dot(linear_part, out_linear, preferred_element_type=jnp.float32) + jnp.dot(attn_part, out_attn, preferred_element_type=jnp.float32)
    return summed.astype(jnp.bfloat16)
```

```python
import functools

import jax
import jax.numpy as jnp
from jax import lax
from jax.experimental import pallas as pl
from jax.experimental.pallas import tpu as pltpu
from jax.sharding import Mesh
from jax.sharding import PartitionSpec as P

HALF = 64
LANES = 128
F32 = jnp.float32
BF16 = jnp.bfloat16
NORM_EPS = 1e-06
GROUP_EPS = 0.00064
LOG2E = 1.4426950408889634
SCORE = HALF ** (-0.5) * LOG2E
FLOOR = -1e29
MASKED = -1e30
STATS = 16
VMEM_LIMIT = 56 * 1024 * 1024


def vmem():
    return pl.BlockSpec(memory_space=pltpu.VMEM)


def smem():
    return pl.BlockSpec(memory_space=pltpu.SMEM)


def params():
    return pltpu.CompilerParams(vmem_limit_bytes=VMEM_LIMIT)


def cost(flops, size):
    return pl.CostEstimate(flops=flops, bytes_accessed=size, transcendentals=0)


def low_lanes(shape=(1, LANES)):
    return lax.broadcasted_iota(jnp.int32, shape, len(shape) - 1) < HALF


def half_sums(v):
    low = low_lanes()
    first = jnp.sum(jnp.where(low, v, 0.0), -1, keepdims=True)
    second = jnp.sum(jnp.where(low, 0.0, v), -1, keepdims=True)
    return jnp.where(low, first, second)


def dot(a, b):
    return jnp.dot(a, b, preferred_element_type=F32)


def dot_nt(a, b):
    return lax.dot_general(a, b, (((1,), (1,)), ((), ())), preferred_element_type=F32)


def dot_tn(a, b):
    return lax.dot_general(a, b, (((0,), (0,)), ((), ())), preferred_element_type=F32)


def two_parts(v):
    high = v.astype(BF16)
    return high, (v - high.astype(F32)).astype(BF16)


def dot3(a, b):
    ah, al = two_parts(a)
    bh, bl = two_parts(b)
    return dot(ah, bh) + (dot(ah, bl) + dot(al, bh))


def rounded(v):
    return v.astype(BF16).astype(F32)


def qkv_kernel(x_ref, gain_ref, wq_ref, wk_ref, wv_ref, qg_ref, kg_ref, normed_ref, q_ref, kv_ref):
    rows = x_ref.shape[0]
    step = 32

    def turn(i, carry):
        span = pl.ds(pl.multiple_of(i * step, step), step)
        x = x_ref[span, :].astype(F32)
        scale = lax.rsqrt(jnp.mean(x * x, -1, keepdims=True) + NORM_EPS)
        normed_ref[span, :] = (x * scale * gain_ref[...]).astype(BF16)
        return carry

    lax.fori_loop(0, rows // step, turn, 0)
    normed = normed_ref[...]

    def map_norm(weight_ref, gain_ref):
        v = rounded(dot(normed, weight_ref[...]))
        scale = lax.rsqrt(half_sums(v * v) * (1.0 / HALF) + NORM_EPS)
        return (v * scale * gain_ref[...]).astype(BF16)

    q_ref[...] = map_norm(wq_ref, qg_ref)
    kv_ref[:, :LANES] = map_norm(wk_ref, kg_ref)
    kv_ref[:, LANES:] = dot(normed, wv_ref[...]).astype(BF16)


def linear_kernel(
    normed_ref,
    wr_ref,
    wk_ref,
    wv_ref,
    wd_ref,
    wg_ref,
    du_ref,
    ru_ref,
    db_ref,
    rb_ref,
    extra_ref,
    extra_t_ref,
    qh_ref,
    ol_ref,
    map_ref,
):
    normed = normed_ref[...]
    length = normed.shape[0]
    low = low_lanes()
    recept = rounded(dot(normed, wr_ref[...]))
    key = rounded(dot(normed, wk_ref[...]))
    value = rounded(dot(normed, wv_ref[...]))
    decay_low = dot(normed, wd_ref[...]).astype(BF16)
    rate_low = dot(normed, wg_ref[...]).astype(BF16)
    log_chan = -jnp.exp(db_ref[...] + jnp.tanh(dot(decay_low, du_ref[...])))
    gate = jax.nn.sigmoid(rb_ref[...] + jnp.tanh(dot(rate_low, ru_ref[...])))
    unit = key * lax.rsqrt(half_sums(key * key) + NORM_EPS)
    extra = extra_ref[...]
    head_step = jnp.where(low, extra[:, 0:1], extra[:, 1:2])
    row = lax.broadcasted_iota(jnp.int32, (length, length), 0)
    col = lax.broadcasted_iota(jnp.int32, (length, length), 1)
    incl = row >= col
    lower = jnp.where(incl, 1.0, 0.0).astype(F32)
    both = jnp.dot(
        lower,
        jnp.concatenate([log_chan, head_step], axis=1),
        preferred_element_type=F32,
        precision=lax.Precision.HIGHEST,
    )
    chan = both[:, :LANES]
    head = both[:, LANES:]
    head_rows = jnp.dot(
        extra_t_ref[...],
        jnp.where(row <= col, 1.0, 0.0).astype(F32),
        preferred_element_type=F32,
        precision=lax.Precision.HIGHEST,
    )
    chan_prev = chan - log_chan
    head_prev = head - head_step
    remove = -unit
    restore = unit * gate
    inject = key * gate
    total = chan + head
    ending = total[length - 1 : length, :]
    to_end = jnp.exp(jnp.minimum(ending - total, 0.0))
    grow = jnp.exp(chan)
    shrink = jnp.exp(-chan)
    left = jnp.concatenate([remove * jnp.exp(chan_prev), recept * grow], axis=0)
    right = jnp.concatenate([restore * shrink, inject * shrink], axis=0).astype(BF16)
    remove_dec = remove * jnp.exp(chan_prev + head_prev)
    recept_dec = recept * jnp.exp(total)
    restore_end = restore * to_end
    inject_end = inject * to_end
    turned = pltpu.roll(value, HALF, 1)
    outs = []
    maps = []
    for h in range(2):
        own = low if h == 0 else jnp.logical_not(low)
        products = dot_nt(jnp.where(own, left, 0.0).astype(BF16), right)
        spread = head[:, h * HALF : h * HALF + 1] - head_rows[h : h + 1, :]
        ratio_incl = jnp.exp(jnp.where(incl, spread, MASKED))
        ratio_strict = jnp.exp(
            jnp.where(row > col, spread - head_step[:, h * HALF : h * HALF + 1], MASKED)
        )
        low_restore = products[:length, :length] * ratio_strict
        low_inject = (products[:length, length:] * ratio_strict).astype(BF16)
        out_restore = (products[length:, :length] * ratio_incl).astype(BF16)
        out_inject = (products[length:, length:] * ratio_incl).astype(BF16)
        inverse = jnp.where(row == col, 1.0, 0.0).astype(F32)
        for level in range((length - 1).bit_length()):
            joint = jnp.right_shift(row, level + 1) == jnp.right_shift(col, level + 1)
            block = joint & (jnp.right_shift(row, level) > jnp.right_shift(col, level))
            part = jnp.where(block, low_restore, 0.0)
            if level == 0:
                inverse = inverse + part
            else:
                known = inverse.astype(BF16)
                inverse = inverse + dot(known, dot(part.astype(BF16), known).astype(BF16))
        other = jnp.where(own, 0.0, turned).astype(BF16)
        sides = jnp.where(own, remove_dec, dot(low_inject, other)).astype(BF16)
        along = dot(inverse.astype(BF16), sides).astype(BF16)
        outs.append(
            dot(out_restore, along) + jnp.where(own, recept_dec, dot(out_inject, other))
        )
        maps.append(
            dot_tn(jnp.where(own, restore_end, 0.0).astype(BF16), along)
            + dot_tn(jnp.where(own, inject_end, 0.0).astype(BF16), other)
        )
    qh_ref[...] = jnp.where(low, outs[0], outs[1]).astype(BF16)
    ol_ref[...] = jnp.where(low, outs[1], outs[0])
    r128 = lax.broadcasted_iota(jnp.int32, (LANES, LANES), 0)
    c128 = lax.broadcasted_iota(jnp.int32, (LANES, LANES), 1)
    map_ref[...] = (
        maps[0] + maps[1] + jnp.where(r128 == c128, jnp.exp(ending) - 1.0, 0.0)
    ).astype(BF16)


def map_masks():
    r = lax.broadcasted_iota(jnp.int32, (LANES, LANES), 0)
    c = lax.broadcasted_iota(jnp.int32, (LANES, LANES), 1)
    same = (r < HALF) == (c < HALF)
    return same, jnp.where(r == c, 1.0, 0.0).astype(F32)


def compose(later, earlier, same):
    return dot3(jnp.where(same, later, 0.0), earlier) + jnp.where(same, 0.0, later)


def row_kernel(place_ref, maps_ref, total_ref, before_ref):
    y = place_ref[1]
    same, eye = map_masks()
    peers, rows, _ = maps_ref.shape
    so_far = eye
    before = eye
    for k in range(peers):
        before = jnp.where(y == k, so_far, before)
        one = maps_ref[k, rows - LANES :, :].astype(F32) + eye
        so_far = one if k == 0 else compose(one, so_far, same)
    before_ref[...] = before
    total_ref[...] = (so_far - eye).astype(BF16)


def carry_kernel(place_ref, totals_ref, before_ref, state_ref):
    z = place_ref[0]
    same, eye = map_masks()
    peers = totals_ref.shape[0]
    level = [
        jnp.where(k < z, totals_ref[k].astype(F32), 0.0) + eye for k in range(peers)
    ]
    while len(level) > 1:
        level = [compose(level[k + 1], level[k], same) for k in range(0, len(level), 2)]
    full = compose(before_ref[...], level[0], same)
    state_ref[...] = jnp.where(same, 0.0, full).astype(BF16)


def attend_kernel(place_ref, q_ref, kv_ref, out_ref, top_ref, acc_ref, wide_ref):
    z = place_ref[0]
    y = place_ref[1]
    rows_q = q_ref.shape[0]
    blk = 256
    span = 1024
    low = low_lanes()
    wide_ref[:, :LANES] = kv_ref[:, LANES:]
    wide_ref[:, LANES:] = jnp.ones((kv_ref.shape[0], LANES), BF16)
    top_ref[...] = jnp.full(top_ref.shape, FLOOR, F32)
    acc_ref[...] = jnp.zeros(acc_ref.shape, F32)

    def step(start, masked):
        keys = kv_ref[pl.ds(start, span), :LANES]
        wide = wide_ref[pl.ds(start, span), :]
        for t in range(rows_q):
            q = q_ref[t, :blk, :]
            if masked:
                row = lax.broadcasted_iota(jnp.int32, (blk, span), 0) + (z * rows_q + t) * blk
                col = lax.broadcasted_iota(jnp.int32, (blk, span), 1)
                k_place = (jnp.right_shift(col, 8) + jnp.right_shift(start, 8)) * rows_q + y
                allowed = row >= k_place * blk + jnp.bitwise_and(col, blk - 1)
            for m in range(2):
                own = low if m == 0 else jnp.logical_not(low)
                s = dot_nt(jnp.where(own, q, jnp.zeros_like(q)), keys) * SCORE
                if masked:
                    s = jnp.where(allowed, s, MASKED)
                at = 2 * t + m
                old = top_ref[at, :, 0:1]
                new = jnp.maximum(old, jnp.max(s, -1, keepdims=True))
                p = jnp.exp2(s - new).astype(BF16)
                acc_ref[at] = acc_ref[at] * jnp.exp2(old - new) + dot(p, wide)
                top_ref[at] = jnp.broadcast_to(new, (blk, LANES))

    whole = (z * blk) // span

    def turn(i, carry):
        step(pl.multiple_of(i * span, span), False)
        return carry

    lax.fori_loop(0, whole, turn, 0)
    step(pl.multiple_of(whole * span, span), True)
    lane = lax.broadcasted_iota(jnp.int32, (1, LANES), 1)
    for t in range(rows_q):
        stats = jnp.zeros((blk, LANES), F32)
        for m in range(2):
            at = 2 * t + m
            acc = acc_ref[at]
            weight = acc[:, LANES : LANES + 1]
            seen = weight > 0.0
            safe = jnp.where(seen, weight, 1.0)
            out_ref[t, :blk, m * LANES : (m + 1) * LANES] = (acc[:, :LANES] / safe).astype(BF16)
            lse = jnp.where(seen, top_ref[at, :, 0:1] + jnp.log2(safe), MASKED)
            high = rounded(lse)
            mid = rounded(lse - high)
            tail = rounded(lse - high - mid)
            stats = jnp.where(lane == m, high, stats)
            stats = jnp.where(lane == 2 + m, mid, stats)
            stats = jnp.where(lane == 4 + m, tail, stats)
        out_ref[t, blk:, :] = stats.T[:STATS, :].astype(BF16)


def finish_kernel(
    lam_ref, parts_ref, hg_ref, qh_ref, ol_ref, state_ref, gg_ref, wl_ref, wa_ref, out_ref
):
    blk = qh_ref.shape[0]
    peers = parts_ref.shape[0]
    lam = lam_ref[0]
    stats = jnp.concatenate(
        [parts_ref[j, blk:, :].astype(F32) for j in range(peers)]
        + [jnp.zeros((LANES - peers * STATS, blk), F32)],
        axis=0,
    ).T
    attended = jnp.zeros((blk, LANES), F32)
    for m in range(2):
        lses = []
        for j in range(peers):
            at = j * STATS + m
            lses.append(
                stats[:, at : at + 1] + stats[:, at + 2 : at + 3] + stats[:, at + 4 : at + 5]
            )
        top = functools.reduce(jnp.maximum, lses)
        shares = [jnp.exp2(v - top) for v in lses]
        whole = functools.reduce(jnp.add, shares)
        mixed = jnp.zeros((blk, LANES), F32)
        for j in range(peers):
            part = parts_ref[j, :blk, m * LANES : (m + 1) * LANES].astype(F32)
            mixed = mixed + part * (shares[j] / whole)
        attended = mixed if m == 0 else attended - lam * mixed
    scale = lax.rsqrt(jnp.mean(attended * attended, -1, keepdims=True) + NORM_EPS)
    attn = (attended * scale * hg_ref[...]).astype(BF16)
    read = dot(qh_ref[...], state_ref[...]) + ol_ref[...]
    centered = read - half_sums(read) * (1.0 / HALF)
    var = half_sums(centered * centered) * (1.0 / HALF)
    linear = centered * lax.rsqrt(var + GROUP_EPS)
    linear = (pltpu.roll(linear, HALF, 1) * gg_ref[...]).astype(BF16)
    width = 512
    for c in range(0, out_ref.shape[1], width):
        out_ref[:, c : c + width] = (
            dot(linear, wl_ref[:, c : c + width]) + dot(attn, wa_ref[:, c : c + width])
        ).astype(BF16)


def copy_for_each(x, axis):
    copies = jnp.broadcast_to(x, (lax.axis_size(axis), *x.shape))
    return lax.all_to_all(copies, axis, split_axis=0, concat_axis=0, tiled=True)


def shards(
    tokens,
    norm_gain,
    recept_weight,
    key_weight,
    value_weight,
    decay_down_weight,
    rate_down,
    decay_up,
    rate_up,
    decay_base,
    rate_base,
    decay_extra,
    group_gain,
    attn_query,
    attn_key,
    attn_value,
    query_gain,
    key_gain,
    lambdas,
    head_gain,
    out_linear,
    out_attn,
):
    shape = jax.ShapeDtypeStruct
    depth = tokens.shape[1]
    peers = lax.axis_size("tp")
    length = tokens.shape[0] * peers
    place = jnp.stack([lax.axis_index("z"), lax.axis_index("y")]).astype(jnp.int32)
    line = lambda v: v.reshape(1, -1)
    rows = copy_for_each(tokens, "tp").reshape(length, depth)
    normed, query, key_value = pl.pallas_call(
        qkv_kernel,
        out_shape=(
            shape((length, depth), BF16),
            shape((length, LANES), BF16),
            shape((length, 2 * LANES), BF16),
        ),
        in_specs=[vmem()] * 7,
        out_specs=(vmem(),) * 3,
        compiler_params=params(),
        cost_estimate=cost(2 * length * depth * 384, 6 << 20),
        name="qkv",
    )(
        rows,
        line(norm_gain),
        attn_query,
        attn_key,
        attn_value,
        line(jnp.tile(query_gain, 2)),
        line(jnp.tile(key_gain, 2)),
    )
    all_kv = lax.all_gather(key_value, "z", axis=0, tiled=True)
    reader, local_out, state_map = pl.pallas_call(
        linear_kernel,
        out_shape=(
            shape((length, LANES), BF16),
            shape((length, LANES), F32),
            shape((LANES, LANES), BF16),
        ),
        in_specs=[vmem()] * 12,
        out_specs=(vmem(),) * 3,
        compiler_params=params(),
        cost_estimate=cost(2 * length * depth * 1024, 6 << 20),
        name="linear",
    )(
        normed,
        recept_weight,
        key_weight,
        value_weight,
        decay_down_weight,
        rate_down,
        decay_up,
        rate_up,
        line(decay_base),
        line(rate_base),
        decay_extra,
        decay_extra.T,
    )
    gathered = lax.all_gather(jnp.concatenate([query, state_map], axis=0), "y")
    total, before = pl.pallas_call(
        row_kernel,
        out_shape=(shape((LANES, LANES), BF16), shape((LANES, LANES), F32)),
        in_specs=[smem(), vmem()],
        out_specs=(vmem(),) * 2,
        compiler_params=params(),
        cost_estimate=cost(1 << 27, 1 << 20),
        name="row",
    )(place, gathered)
    totals = lax.all_gather(total, "z")
    state = pl.pallas_call(
        carry_kernel,
        out_shape=shape((LANES, LANES), BF16),
        in_specs=[smem(), vmem(), vmem()],
        out_specs=vmem(),
        compiler_params=params(),
        cost_estimate=cost(1 << 27, 1 << 20),
        name="carry",
    )(place, totals, before)
    all_kv, state = lax.optimization_barrier((all_kv, state))
    rows_q = gathered.shape[0]
    partial = pl.pallas_call(
        attend_kernel,
        out_shape=shape((rows_q, length + STATS, 2 * LANES), BF16),
        in_specs=[smem(), vmem(), vmem()],
        out_specs=vmem(),
        scratch_shapes=[
            pltpu.VMEM((2 * rows_q, length, LANES), F32),
            pltpu.VMEM((2 * rows_q, length, 2 * LANES), F32),
            pltpu.VMEM((all_kv.shape[0], 2 * LANES), BF16),
        ],
        compiler_params=params(),
        cost_estimate=cost(4 * rows_q * length * all_kv.shape[0] * 384, 6 << 20),
        name="attend",
    )(place, gathered, all_kv)
    parts = lax.all_to_all(partial, "y", split_axis=0, concat_axis=0, tiled=True)
    share = pl.pallas_call(
        finish_kernel,
        out_shape=shape((length, depth), BF16),
        in_specs=[smem()] + [vmem()] * 8,
        out_specs=vmem(),
        compiler_params=params(),
        cost_estimate=cost(2 * length * depth * 256, 4 << 20),
        name="finish",
    )(
        lambdas,
        parts,
        line(head_gain),
        reader,
        local_out,
        state,
        line(group_gain),
        out_linear,
        out_attn,
    )
    arrived = lax.all_to_all(
        share.reshape(peers, length // peers, depth), "tp", split_axis=0, concat_axis=0, tiled=True
    )
    return arrived.astype(F32).sum(axis=0).astype(BF16)


def solution(mesh):
    torus = Mesh(mesh.devices.reshape(16, 4, mesh.shape["tp"]), ("z", "y", "tp"))
    seq = ("z", "y")
    return jax.shard_map(
        shards,
        mesh=torus,
        in_specs=(
            P(("z", "y", "tp"), None),
            P(),
            P(None, "tp"),
            P(None, "tp"),
            P(None, "tp"),
            P(),
            P(),
            P(None, "tp"),
            P(None, "tp"),
            P("tp"),
            P("tp"),
            P(seq, "tp"),
            P("tp"),
            P(None, "tp"),
            P(None, "tp"),
            P(None, "tp"),
            P(),
            P(),
            P("tp"),
            P(),
            P("tp", None),
            P("tp", None),
        ),
        out_specs=P(("z", "y", "tp"), None),
        check_vma=False,
    )
```

```python
import functools

import jax
import jax.numpy as jnp
from jax import lax
from jax.experimental import pallas as pl
from jax.experimental.pallas import tpu as pltpu
from jax.sharding import Mesh
from jax.sharding import PartitionSpec as P

HALF = 64
LANES = 128
F32 = jnp.float32
BF16 = jnp.bfloat16
NORM_EPS = 1e-06
GROUP_EPS = 0.00064
LOG2E = 1.4426950408889634
SCORE = HALF ** (-0.5) * LOG2E
FLOOR = -1e29
MASKED = -1e30
STATS = 16
VMEM_LIMIT = 56 * 1024 * 1024


def vmem():
    return pl.BlockSpec(memory_space=pltpu.VMEM)


def smem():
    return pl.BlockSpec(memory_space=pltpu.SMEM)


def params():
    return pltpu.CompilerParams(vmem_limit_bytes=VMEM_LIMIT)


def cost(flops, size):
    return pl.CostEstimate(flops=flops, bytes_accessed=size, transcendentals=0)


def low_lanes(shape=(1, LANES)):
    return lax.broadcasted_iota(jnp.int32, shape, len(shape) - 1) < HALF


def half_sums(v):
    low = low_lanes()
    first = jnp.sum(jnp.where(low, v, 0.0), -1, keepdims=True)
    second = jnp.sum(jnp.where(low, 0.0, v), -1, keepdims=True)
    return jnp.where(low, first, second)


def dot(a, b):
    return jnp.dot(a, b, preferred_element_type=F32)


def dot_nt(a, b):
    return lax.dot_general(a, b, (((1,), (1,)), ((), ())), preferred_element_type=F32)


def dot_tn(a, b):
    return lax.dot_general(a, b, (((0,), (0,)), ((), ())), preferred_element_type=F32)


def two_parts(v):
    high = v.astype(BF16)
    return high, (v - high.astype(F32)).astype(BF16)


def dot3(a, b):
    ah, al = two_parts(a)
    bh, bl = two_parts(b)
    return dot(ah, bh) + (dot(ah, bl) + dot(al, bh))


def rounded(v):
    return v.astype(BF16).astype(F32)


def qkv_kernel(
    mine_ref, other_ref, gain_ref, wq_ref, wk_ref, wv_ref, qg_ref, kg_ref, normed_ref, q_ref, kv_ref
):
    core = lax.axis_index("c")
    chips, step, _ = mine_ref.shape

    def turn(i, carry):
        for source, at in ((mine_ref, 2 * i + core), (other_ref, 2 * i + 1 - core)):
            x = source[i].astype(F32)
            scale = lax.rsqrt(jnp.mean(x * x, -1, keepdims=True) + NORM_EPS)
            span = pl.ds(pl.multiple_of(at * step, step), step)
            normed_ref[span, :] = (x * scale * gain_ref[...]).astype(BF16)
        return carry

    lax.fori_loop(0, chips, turn, 0)
    normed = normed_ref[...]

    def map_norm(weight_ref, gain_ref):
        v = rounded(dot(normed, weight_ref[...]))
        scale = lax.rsqrt(half_sums(v * v) * (1.0 / HALF) + NORM_EPS)
        return (v * scale * gain_ref[...]).astype(BF16)

    q_ref[...] = map_norm(wq_ref, qg_ref)
    kv_ref[:, :LANES] = map_norm(wk_ref, kg_ref)
    kv_ref[:, LANES:] = dot(normed, wv_ref[...]).astype(BF16)


def linear_kernel(
    normed_ref,
    q_ref,
    wr_ref,
    wk_ref,
    wv_ref,
    wd_ref,
    wg_ref,
    du_ref,
    ru_ref,
    db_ref,
    rb_ref,
    extra_t_ref,
    qh_ref,
    ol_ref,
    pay_ref,
):
    normed = normed_ref[...]
    length = normed.shape[0]
    low = low_lanes()
    recept = rounded(dot(normed, wr_ref[...]))
    key = rounded(dot(normed, wk_ref[...]))
    value = rounded(dot(normed, wv_ref[...]))
    decay_low = dot_nt(normed, wd_ref[...]).astype(BF16)
    rate_low = dot_nt(normed, wg_ref[...]).astype(BF16)
    log_chan = -jnp.exp(db_ref[...] + jnp.tanh(dot(decay_low, du_ref[...])))
    gate = jax.nn.sigmoid(rb_ref[...] + jnp.tanh(dot(rate_low, ru_ref[...])))
    unit = key * lax.rsqrt(half_sums(key * key) + NORM_EPS)
    head_step = jnp.concatenate(
        [jnp.broadcast_to(extra_t_ref[h : h + 1, :], (HALF, length)) for h in range(2)], axis=0
    ).T
    row = lax.broadcasted_iota(jnp.int32, (length, length), 0)
    col = lax.broadcasted_iota(jnp.int32, (length, length), 1)
    incl = row >= col
    lower = jnp.where(incl, 1.0, 0.0).astype(F32)
    both = jnp.dot(
        lower,
        jnp.concatenate([log_chan, head_step], axis=1),
        preferred_element_type=F32,
        precision=lax.Precision.HIGHEST,
    )
    chan = both[:, :LANES]
    head = both[:, LANES:]
    head_rows = jnp.dot(
        extra_t_ref[...],
        jnp.where(row <= col, 1.0, 0.0).astype(F32),
        preferred_element_type=F32,
        precision=lax.Precision.HIGHEST,
    )
    chan_prev = chan - log_chan
    head_prev = head - head_step
    remove = -unit
    restore = unit * gate
    inject = key * gate
    total = chan + head
    ending = total[length - 1 : length, :]
    to_end = jnp.exp(jnp.minimum(ending - total, 0.0))
    grow = jnp.exp(chan)
    shrink = jnp.exp(-chan)
    left = jnp.concatenate([remove * jnp.exp(chan_prev), recept * grow], axis=0)
    right = jnp.concatenate([restore * shrink, inject * shrink], axis=0).astype(BF16)
    remove_dec = remove * jnp.exp(chan_prev + head_prev)
    recept_dec = recept * jnp.exp(total)
    restore_end = restore * to_end
    inject_end = inject * to_end
    turned = pltpu.roll(value, HALF, 1)
    outs = []
    maps = []
    for h in range(2):
        own = low if h == 0 else jnp.logical_not(low)
        products = dot_nt(jnp.where(own, left, 0.0).astype(BF16), right)
        spread = head[:, h * HALF : h * HALF + 1] - head_rows[h : h + 1, :]
        ratio_incl = jnp.exp(jnp.where(incl, spread, MASKED))
        ratio_strict = jnp.exp(
            jnp.where(row > col, spread - head_step[:, h * HALF : h * HALF + 1], MASKED)
        )
        low_restore = products[:length, :length] * ratio_strict
        low_inject = (products[:length, length:] * ratio_strict).astype(BF16)
        out_restore = (products[length:, :length] * ratio_incl).astype(BF16)
        out_inject = (products[length:, length:] * ratio_incl).astype(BF16)
        inverse = jnp.where(row == col, 1.0, 0.0).astype(F32)
        for level in range((length - 1).bit_length()):
            joint = jnp.right_shift(row, level + 1) == jnp.right_shift(col, level + 1)
            block = joint & (jnp.right_shift(row, level) > jnp.right_shift(col, level))
            part = jnp.where(block, low_restore, 0.0)
            if level == 0:
                inverse = inverse + part
            else:
                known = inverse.astype(BF16)
                inverse = inverse + dot(known, dot(part.astype(BF16), known).astype(BF16))
        other = jnp.where(own, 0.0, turned).astype(BF16)
        sides = jnp.where(own, remove_dec, dot(low_inject, other)).astype(BF16)
        along = dot(inverse.astype(BF16), sides).astype(BF16)
        outs.append(
            dot(out_restore, along) + jnp.where(own, recept_dec, dot(out_inject, other))
        )
        maps.append(
            dot_tn(jnp.where(own, restore_end, 0.0).astype(BF16), along)
            + dot_tn(jnp.where(own, inject_end, 0.0).astype(BF16), other)
        )
    qh_ref[...] = jnp.where(low, outs[0], outs[1]).astype(BF16)
    ol_ref[...] = jnp.where(low, outs[1], outs[0])
    r128 = lax.broadcasted_iota(jnp.int32, (LANES, LANES), 0)
    c128 = lax.broadcasted_iota(jnp.int32, (LANES, LANES), 1)
    pay_ref[:length, :] = q_ref[...]
    pay_ref[length:, :] = (
        maps[0] + maps[1] + jnp.where(r128 == c128, jnp.exp(ending) - 1.0, 0.0)
    ).astype(BF16)


def map_masks():
    r = lax.broadcasted_iota(jnp.int32, (LANES, LANES), 0)
    c = lax.broadcasted_iota(jnp.int32, (LANES, LANES), 1)
    same = (r < HALF) == (c < HALF)
    return same, jnp.where(r == c, 1.0, 0.0).astype(F32)


def compose(later, earlier, same):
    return dot3(jnp.where(same, later, 0.0), earlier) + jnp.where(same, 0.0, later)


def row_kernel(maps_ref, total_ref, before_ref):
    y = lax.axis_index("y")
    same, eye = map_masks()
    peers, rows, _ = maps_ref.shape
    so_far = eye
    before = eye
    for k in range(peers):
        before = jnp.where(y == k, so_far, before)
        one = maps_ref[k, rows - LANES :, :].astype(F32) + eye
        so_far = one if k == 0 else compose(one, so_far, same)
    before_ref[...] = before
    total_ref[...] = (so_far - eye).astype(BF16)


def carry_kernel(totals_ref, before_ref, state_ref):
    z = lax.axis_index("z")
    same, eye = map_masks()
    peers = totals_ref.shape[0]
    level = [
        jnp.where(k < z, totals_ref[k].astype(F32), 0.0) + eye for k in range(peers)
    ]
    while len(level) > 1:
        level = [compose(level[k + 1], level[k], same) for k in range(0, len(level), 2)]
    full = compose(before_ref[...], level[0], same)
    state_ref[...] = jnp.where(same, 0.0, full).astype(BF16)


def attend_kernel(q_ref, kv_ref, out_ref, top_ref, acc_ref, wide_ref):
    z = lax.axis_index("z")
    y = lax.axis_index("y")
    rows_q = q_ref.shape[0]
    blk = top_ref.shape[1]
    span = 4 * blk
    low = low_lanes()
    wide_ref[:, :LANES] = kv_ref[:, LANES:]
    wide_ref[:, LANES:] = jnp.ones((kv_ref.shape[0], LANES), BF16)
    top_ref[...] = jnp.full(top_ref.shape, FLOOR, F32)
    acc_ref[...] = jnp.zeros(acc_ref.shape, F32)

    def step(index, masked):
        start = pl.multiple_of(index * span, span)
        keys = kv_ref[pl.ds(start, span), :LANES]
        wide = wide_ref[pl.ds(start, span), :]

        def scores(at):
            own = low if at % 2 == 0 else jnp.logical_not(low)
            q = q_ref[at // 2, :blk, :]
            return dot_nt(jnp.where(own, q, jnp.zeros_like(q)), keys)

        if masked:
            row = lax.broadcasted_iota(jnp.int32, (blk, span), 0)
            col = lax.broadcasted_iota(jnp.int32, (blk, span), 1)
            k_place = (jnp.right_shift(col, 8) + index * 4) * rows_q + y
            behind = (k_place - z * rows_q) * blk + jnp.bitwise_and(col, blk - 1) - row
        ahead = [scores(at) for at in range(1)]
        for at in range(2 * rows_q):
            if at + 1 < 2 * rows_q:
                ahead.append(scores(at + 1))
            s = ahead.pop(0) * SCORE
            if masked:
                s = jnp.where(behind <= (at // 2) * blk, s, MASKED)
            if False:
                p = jnp.exp2(s).astype(BF16)
                acc_ref[at] = acc_ref[at] + dot(p, wide)
                continue
            old = top_ref[at, :, 0:1]
            new = jnp.maximum(old, jnp.max(s, -1, keepdims=True))
            p = jnp.exp2(s - new).astype(BF16)
            acc_ref[at] = acc_ref[at] * jnp.exp2(old - new) + dot(p, wide)
            top_ref[at] = jnp.broadcast_to(new, (blk, LANES))

    whole = lax.div(z, 4)

    def turn(i, carry):
        step(i, False)
        return carry

    lax.fori_loop(0, whole, turn, 0)
    step(whole, True)
    lane = lax.broadcasted_iota(jnp.int32, (1, LANES), 1)
    for t in range(rows_q):
        stats = jnp.zeros((blk, LANES), F32)
        for m in range(2):
            at = 2 * t + m
            acc = acc_ref[at]
            weight = acc[:, LANES : LANES + 1]
            seen = weight > 0.0
            safe = jnp.where(seen, weight, 1.0)
            out_ref[t, :blk, m * LANES : (m + 1) * LANES] = (acc[:, :LANES] / safe).astype(BF16)
            lse = jnp.where(seen, top_ref[at, :, 0:1] + jnp.log2(safe), MASKED)
            high = rounded(lse)
            mid = rounded(lse - high)
            tail = rounded(lse - high - mid)
            stats = jnp.where(lane == m, high, stats)
            stats = jnp.where(lane == 2 + m, mid, stats)
            stats = jnp.where(lane == 4 + m, tail, stats)
        out_ref[t, blk:, :] = stats.T[:STATS, :].astype(BF16)


def finish_kernel(
    lam_ref, parts_ref, hg_ref, qh_ref, ol_ref, state_ref, gg_ref, wl_ref, wa_ref, out_ref
):
    blk = qh_ref.shape[0]
    peers = parts_ref.shape[0]
    lam = lam_ref[0]
    stats = jnp.concatenate(
        [parts_ref[j, blk:, :].astype(F32) for j in range(peers)]
        + [jnp.zeros((LANES - peers * STATS, blk), F32)],
        axis=0,
    ).T
    attended = jnp.zeros((blk, LANES), F32)
    for m in range(2):
        lses = []
        for j in range(peers):
            at = j * STATS + m
            lses.append(
                stats[:, at : at + 1] + stats[:, at + 2 : at + 3] + stats[:, at + 4 : at + 5]
            )
        top = functools.reduce(jnp.maximum, lses)
        shares = [jnp.exp2(v - top) for v in lses]
        whole = functools.reduce(jnp.add, shares)
        mixed = jnp.zeros((blk, LANES), F32)
        for j in range(peers):
            part = parts_ref[j, :blk, m * LANES : (m + 1) * LANES].astype(F32)
            mixed = mixed + part * (shares[j] / whole)
        attended = mixed if m == 0 else attended - lam * mixed
    scale = lax.rsqrt(jnp.mean(attended * attended, -1, keepdims=True) + NORM_EPS)
    attn = (attended * scale * hg_ref[...]).astype(BF16)
    read = dot(qh_ref[...], state_ref[...]) + ol_ref[...]
    centered = read - half_sums(read) * (1.0 / HALF)
    var = half_sums(centered * centered) * (1.0 / HALF)
    linear = centered * lax.rsqrt(var + GROUP_EPS)
    linear = (pltpu.roll(linear, HALF, 1) * gg_ref[...]).astype(BF16)
    width = 512
    for c in range(0, out_ref.shape[1], width):
        out_ref[:, c : c + width] = (
            dot(linear, wl_ref[:, c : c + width]) + dot(attn, wa_ref[:, c : c + width])
        ).astype(BF16)


def swap_cores(x):
    return lax.ppermute(x, "c", [(0, 1), (1, 0)])


def shards(
    tokens,
    norm_gain,
    recept_weight,
    key_weight,
    value_weight,
    decay_down_weight,
    rate_down,
    decay_up,
    rate_up,
    decay_base,
    rate_base,
    decay_extra,
    group_gain,
    attn_query,
    attn_key,
    attn_value,
    query_gain,
    key_gain,
    lambdas,
    head_gain,
    out_linear,
    out_attn,
):
    shape = jax.ShapeDtypeStruct
    depth = tokens.shape[1]
    peers = lax.axis_size("x") * lax.axis_size("c")
    length = tokens.shape[0] * peers
    line = lambda v: v.reshape(1, -1)
    mine = lax.all_gather(tokens, "x")
    other = swap_cores(mine)
    normed, query, key_value = pl.pallas_call(
        qkv_kernel,
        out_shape=(
            shape((length, depth), BF16),
            shape((length, LANES), BF16),
            shape((length, 2 * LANES), BF16),
        ),
        in_specs=[vmem()] * 8,
        out_specs=(vmem(),) * 3,
        compiler_params=params(),
        cost_estimate=cost(2 * length * depth * 384, 6 << 20),
        name="qkv",
    )(
        mine,
        other,
        line(norm_gain),
        attn_query,
        attn_key,
        attn_value,
        line(jnp.tile(query_gain, 2)),
        line(jnp.tile(key_gain, 2)),
    )
    all_kv = lax.all_gather(key_value, "z", axis=0, tiled=True)
    reader, local_out, payload = pl.pallas_call(
        linear_kernel,
        out_shape=(
            shape((length, LANES), BF16),
            shape((length, LANES), F32),
            shape((length + LANES, LANES), BF16),
        ),
        in_specs=[vmem()] * 12,
        out_specs=(vmem(),) * 3,
        compiler_params=params(),
        cost_estimate=cost(2 * length * depth * 1024, 6 << 20),
        name="linear",
    )(
        normed,
        query,
        recept_weight,
        key_weight,
        value_weight,
        decay_down_weight.T,
        rate_down.T,
        decay_up,
        rate_up,
        line(decay_base),
        line(rate_base),
        decay_extra.T,
    )
    gathered = lax.all_gather(payload, "y")
    total, before = pl.pallas_call(
        row_kernel,
        out_shape=(shape((LANES, LANES), BF16), shape((LANES, LANES), F32)),
        in_specs=[vmem()],
        out_specs=(vmem(),) * 2,
        compiler_params=params(),
        cost_estimate=cost(1 << 27, 1 << 20),
        name="row",
    )(gathered)
    totals = lax.all_gather(total, "z")
    state = pl.pallas_call(
        carry_kernel,
        out_shape=shape((LANES, LANES), BF16),
        in_specs=[vmem(), vmem()],
        out_specs=vmem(),
        compiler_params=params(),
        cost_estimate=cost(1 << 27, 1 << 20),
        name="carry",
    )(totals, before)
    all_kv, state = lax.optimization_barrier((all_kv, state))
    rows_q = gathered.shape[0]
    partial = pl.pallas_call(
        attend_kernel,
        out_shape=shape((rows_q, length + STATS, 2 * LANES), BF16),
        in_specs=[vmem(), vmem()],
        out_specs=vmem(),
        scratch_shapes=[
            pltpu.VMEM((2 * rows_q, length, LANES), F32),
            pltpu.VMEM((2 * rows_q, length, 2 * LANES), F32),
            pltpu.VMEM((all_kv.shape[0], 2 * LANES), BF16),
        ],
        compiler_params=params(),
        cost_estimate=cost(4 * rows_q * length * all_kv.shape[0] * 384, 6 << 20),
        name="attend",
    )(gathered, all_kv)
    parts = lax.all_to_all(partial, "y", split_axis=0, concat_axis=0, tiled=True)
    share = pl.pallas_call(
        finish_kernel,
        out_shape=shape((length, depth), BF16),
        in_specs=[smem()] + [vmem()] * 8,
        out_specs=vmem(),
        compiler_params=params(),
        cost_estimate=cost(2 * length * depth * 256, 4 << 20),
        name="finish",
    )(
        lambdas,
        parts,
        line(head_gain),
        reader,
        local_out,
        state,
        line(group_gain),
        out_linear,
        out_attn,
    )
    arrived = lax.all_to_all(
        share.reshape(peers, length // peers, depth),
        ("x", "c"),
        split_axis=0,
        concat_axis=0,
        tiled=True,
    )
    return arrived.astype(F32).sum(axis=0).astype(BF16)


def solution(mesh):
    torus = Mesh(mesh.devices.reshape(16, 4, 4, 2), ("z", "y", "x", "c"))
    seq = ("z", "y")
    tp = ("x", "c")
    every = P(seq + tp, None)
    return jax.shard_map(
        shards,
        mesh=torus,
        in_specs=(
            every,
            P(),
            P(None, tp),
            P(None, tp),
            P(None, tp),
            P(),
            P(),
            P(None, tp),
            P(None, tp),
            P(tp),
            P(tp),
            P(seq, tp),
            P(tp),
            P(None, tp),
            P(None, tp),
            P(None, tp),
            P(),
            P(),
            P(tp),
            P(),
            P(tp, None),
            P(tp, None),
        ),
        out_specs=every,
        check_vma=False,
    )
```

```python
import functools

import jax
import jax.numpy as jnp
from jax import lax
from jax.experimental import pallas as pl
from jax.experimental.pallas import tpu as pltpu
from jax.sharding import Mesh
from jax.sharding import PartitionSpec as P

HALF = 64
LANES = 128
F32 = jnp.float32
BF16 = jnp.bfloat16
NORM_EPS = 1e-06
GROUP_EPS = 0.00064
LOG2E = 1.4426950408889634
SCORE = HALF ** (-0.5) * LOG2E
FLOOR = -1e29
MASKED = -1e30
STATS = 16


def vmem():
    return pl.BlockSpec(memory_space=pltpu.VMEM)


def smem():
    return pl.BlockSpec(memory_space=pltpu.SMEM)


def params(mib):
    return pltpu.CompilerParams(vmem_limit_bytes=mib << 20)


def cost(flops, size):
    return pl.CostEstimate(flops=flops, bytes_accessed=size, transcendentals=0)


def low_lanes(shape=(1, LANES)):
    return lax.broadcasted_iota(jnp.int32, shape, len(shape) - 1) < HALF


def half_sums(v):
    low = low_lanes()
    first = jnp.sum(jnp.where(low, v, 0.0), -1, keepdims=True)
    second = jnp.sum(jnp.where(low, 0.0, v), -1, keepdims=True)
    return jnp.where(low, first, second)


def dot(a, b):
    return jnp.dot(a, b, preferred_element_type=F32)


def dot_nt(a, b):
    return lax.dot_general(a, b, (((1,), (1,)), ((), ())), preferred_element_type=F32)


def dot_tn(a, b):
    return lax.dot_general(a, b, (((0,), (0,)), ((), ())), preferred_element_type=F32)


def two_parts(v):
    high = v.astype(BF16)
    return high, (v - high.astype(F32)).astype(BF16)


def dot3(a, b):
    ah, al = two_parts(a)
    bh, bl = two_parts(b)
    return dot(ah, bh) + (dot(ah, bl) + dot(al, bh))


def rounded(v):
    return v.astype(BF16).astype(F32)


def qkv_kernel(
    mine_ref, other_ref, gain_ref, wq_ref, wk_ref, wv_ref, qg_ref, kg_ref, normed_ref, q_ref, kv_ref
):
    core = lax.axis_index("c")
    chips, step, _ = mine_ref.shape

    def turn(i, carry):
        for source, at in ((mine_ref, 2 * i + core), (other_ref, 2 * i + 1 - core)):
            x = source[i].astype(F32)
            scale = lax.rsqrt(jnp.mean(x * x, -1, keepdims=True) + NORM_EPS)
            span = pl.ds(pl.multiple_of(at * step, step), step)
            normed_ref[span, :] = (x * scale * gain_ref[...]).astype(BF16)
        return carry

    lax.fori_loop(0, chips, turn, 0)
    normed = normed_ref[...]

    def map_norm(weight_ref, gain_ref):
        v = rounded(dot(normed, weight_ref[...]))
        scale = lax.rsqrt(half_sums(v * v) * (1.0 / HALF) + NORM_EPS)
        return (v * scale * gain_ref[...]).astype(BF16)

    q_ref[...] = map_norm(wq_ref, qg_ref)
    kv_ref[:, :LANES] = map_norm(wk_ref, kg_ref)
    kv_ref[:, LANES:] = dot(normed, wv_ref[...]).astype(BF16)


def linear_kernel(
    normed_ref,
    q_ref,
    wr_ref,
    wk_ref,
    wv_ref,
    wd_ref,
    wg_ref,
    du_ref,
    ru_ref,
    db_ref,
    rb_ref,
    extra_t_ref,
    qh_ref,
    ol_ref,
    pay_ref,
):
    normed = normed_ref[...]
    length = normed.shape[0]
    low = low_lanes()
    recept = rounded(dot(normed, wr_ref[...]))
    key = rounded(dot(normed, wk_ref[...]))
    value = rounded(dot(normed, wv_ref[...]))
    decay_low = dot_nt(normed, wd_ref[...]).astype(BF16)
    rate_low = dot_nt(normed, wg_ref[...]).astype(BF16)
    log_chan = -jnp.exp(db_ref[...] + jnp.tanh(dot(decay_low, du_ref[...])))
    gate = jax.nn.sigmoid(rb_ref[...] + jnp.tanh(dot(rate_low, ru_ref[...])))
    unit = key * lax.rsqrt(half_sums(key * key) + NORM_EPS)
    head_step = jnp.concatenate(
        [jnp.broadcast_to(extra_t_ref[h : h + 1, :], (HALF, length)) for h in range(2)], axis=0
    ).T
    row = lax.broadcasted_iota(jnp.int32, (length, length), 0)
    col = lax.broadcasted_iota(jnp.int32, (length, length), 1)
    incl = row >= col
    lower = jnp.where(incl, 1.0, 0.0).astype(F32)
    both = jnp.dot(
        lower,
        jnp.concatenate([log_chan, head_step], axis=1),
        preferred_element_type=F32,
        precision=lax.Precision.HIGHEST,
    )
    chan = both[:, :LANES]
    head = both[:, LANES:]
    head_rows = jnp.dot(
        extra_t_ref[...],
        jnp.where(row <= col, 1.0, 0.0).astype(F32),
        preferred_element_type=F32,
        precision=lax.Precision.HIGHEST,
    )
    chan_prev = chan - log_chan
    head_prev = head - head_step
    remove = -unit
    restore = unit * gate
    inject = key * gate
    total = chan + head
    ending = total[length - 1 : length, :]
    to_end = jnp.exp(jnp.minimum(ending - total, 0.0))
    grow = jnp.exp(chan)
    shrink = jnp.exp(-chan)
    left = jnp.concatenate([remove * jnp.exp(chan_prev), recept * grow], axis=0)
    right = jnp.concatenate([restore * shrink, inject * shrink], axis=0).astype(BF16)
    remove_dec = remove * jnp.exp(chan_prev + head_prev)
    recept_dec = recept * jnp.exp(total)
    restore_end = restore * to_end
    inject_end = inject * to_end
    turned = pltpu.roll(value, HALF, 1)
    outs = []
    maps = []
    for h in range(2):
        own = low if h == 0 else jnp.logical_not(low)
        products = dot_nt(jnp.where(own, left, 0.0).astype(BF16), right)
        spread = head[:, h * HALF : h * HALF + 1] - head_rows[h : h + 1, :]
        ratio_incl = jnp.exp(jnp.where(incl, spread, MASKED))
        ratio_strict = jnp.exp(
            jnp.where(row > col, spread - head_step[:, h * HALF : h * HALF + 1], MASKED)
        )
        low_restore = products[:length, :length] * ratio_strict
        low_inject = (products[:length, length:] * ratio_strict).astype(BF16)
        out_restore = (products[length:, :length] * ratio_incl).astype(BF16)
        out_inject = (products[length:, length:] * ratio_incl).astype(BF16)
        inverse = jnp.where(row == col, 1.0, 0.0).astype(F32)
        for level in range((length - 1).bit_length()):
            joint = jnp.right_shift(row, level + 1) == jnp.right_shift(col, level + 1)
            block = joint & (jnp.right_shift(row, level) > jnp.right_shift(col, level))
            part = jnp.where(block, low_restore, 0.0)
            if level == 0:
                inverse = inverse + part
            else:
                known = inverse.astype(BF16)
                inverse = inverse + dot(known, dot(part.astype(BF16), known).astype(BF16))
        other = jnp.where(own, 0.0, turned).astype(BF16)
        sides = jnp.where(own, remove_dec, dot(low_inject, other)).astype(BF16)
        along = dot(inverse.astype(BF16), sides).astype(BF16)
        outs.append(
            dot(out_restore, along) + jnp.where(own, recept_dec, dot(out_inject, other))
        )
        maps.append(
            dot_tn(jnp.where(own, restore_end, 0.0).astype(BF16), along)
            + dot_tn(jnp.where(own, inject_end, 0.0).astype(BF16), other)
        )
    qh_ref[...] = jnp.where(low, outs[0], outs[1]).astype(BF16)
    ol_ref[...] = jnp.where(low, outs[1], outs[0])
    r128 = lax.broadcasted_iota(jnp.int32, (LANES, LANES), 0)
    c128 = lax.broadcasted_iota(jnp.int32, (LANES, LANES), 1)
    pay_ref[:length, :] = q_ref[...]
    pay_ref[length:, :] = (
        maps[0] + maps[1] + jnp.where(r128 == c128, jnp.exp(ending) - 1.0, 0.0)
    ).astype(BF16)


def map_masks():
    r = lax.broadcasted_iota(jnp.int32, (LANES, LANES), 0)
    c = lax.broadcasted_iota(jnp.int32, (LANES, LANES), 1)
    same = (r < HALF) == (c < HALF)
    return same, jnp.where(r == c, 1.0, 0.0).astype(F32)


def compose(later, earlier, same):
    return dot3(jnp.where(same, later, 0.0), earlier) + jnp.where(same, 0.0, later)


def row_kernel(maps_ref, total_ref, before_ref):
    y = lax.axis_index("y")
    same, eye = map_masks()
    peers, rows, _ = maps_ref.shape
    so_far = eye
    before = eye
    for k in range(peers):
        before = jnp.where(y == k, so_far, before)
        one = maps_ref[k, rows - LANES :, :].astype(F32) + eye
        so_far = one if k == 0 else compose(one, so_far, same)
    before_ref[...] = before
    total_ref[...] = (so_far - eye).astype(BF16)


def carry_kernel(totals_ref, before_ref, state_ref):
    z = lax.axis_index("z")
    same, eye = map_masks()
    peers = totals_ref.shape[0]
    level = [
        jnp.where(k < z, totals_ref[k].astype(F32), 0.0) + eye for k in range(peers)
    ]
    while len(level) > 1:
        level = [compose(level[k + 1], level[k], same) for k in range(0, len(level), 2)]
    full = compose(before_ref[...], level[0], same)
    state_ref[...] = jnp.where(same, 0.0, full).astype(BF16)


def attend_kernel(q_ref, kv_hbm, out_ref, top_ref, acc_ref, kv_ref, wide_ref, sems):
    z = lax.axis_index("z")
    y = lax.axis_index("y")
    rows_q = q_ref.shape[0]
    blk = top_ref.shape[1]
    group = 4
    span = group * blk
    low = low_lanes()
    whole = lax.div(z, group)

    def fetch(index):
        at = pl.ds(pl.multiple_of(index * span, span), span)
        return pltpu.make_async_copy(kv_hbm.at[at, :], kv_ref.at[at, :], sems.at[index])

    fetch(whole).start()

    def begin(i, carry):
        fetch(i).start()
        return carry

    lax.fori_loop(0, whole, begin, 0)
    wide_ref[:, LANES:] = jnp.ones((span, LANES), BF16)

    def step(index, last):
        fetch(index).wait()
        at_keys = pl.ds(pl.multiple_of(index * span, span), span)
        keys = kv_ref[at_keys, :LANES]
        wide_ref[:, :LANES] = kv_ref[at_keys, LANES:]
        wide = wide_ref[...]

        def scores(at):
            own = low if at % 2 == 0 else jnp.logical_not(low)
            q = q_ref[at // 2, :blk, :]
            return dot_nt(jnp.where(own, q, jnp.zeros_like(q)), keys)

        if last:
            row = lax.broadcasted_iota(jnp.int32, (blk, span), 0)
            col = lax.broadcasted_iota(jnp.int32, (blk, span), 1)
            k_place = (jnp.right_shift(col, 8) + index * group) * rows_q + y
            behind = (k_place - z * rows_q) * blk + jnp.bitwise_and(col, blk - 1) - row
        ahead = scores(0)
        for at in range(2 * rows_q):
            s = ahead * SCORE
            if at + 1 < 2 * rows_q:
                ahead = scores(at + 1)
            if last:
                s = jnp.where(behind <= (at // 2) * blk, s, MASKED)
                new = jnp.maximum(jnp.max(s, -1, keepdims=True), FLOOR)
                acc_ref[at] = dot(jnp.exp2(s - new).astype(BF16), wide)
            else:
                old = top_ref[at, :, 0:1]
                new = jnp.maximum(old, jnp.max(s, -1, keepdims=True))
                p = jnp.exp2(s - new).astype(BF16)
                acc_ref[at] = acc_ref[at] * jnp.exp2(old - new) + dot(p, wide)
            top_ref[at] = jnp.broadcast_to(new, (blk, LANES))

    step(whole, True)

    def turn(i, carry):
        step(i, False)
        return carry

    lax.fori_loop(0, whole, turn, 0)
    lane = lax.broadcasted_iota(jnp.int32, (1, LANES), 1)
    for t in range(rows_q):
        stats = jnp.zeros((blk, LANES), F32)
        for m in range(2):
            at = 2 * t + m
            acc = acc_ref[at]
            weight = acc[:, LANES:]
            seen = weight > 0.0
            safe = jnp.where(seen, weight, 1.0)
            out_ref[t, :blk, m * LANES : (m + 1) * LANES] = (acc[:, :LANES] / safe).astype(BF16)
            lse = jnp.where(seen, top_ref[at] + jnp.log2(safe), MASKED)
            high = rounded(lse)
            mid = rounded(lse - high)
            tail = rounded(lse - high - mid)
            stats = jnp.where(lane == m, high, stats)
            stats = jnp.where(lane == 2 + m, mid, stats)
            stats = jnp.where(lane == 4 + m, tail, stats)
        out_ref[t, blk:, :] = stats.T[:STATS, :].astype(BF16)


def finish_kernel(
    lam_ref, parts_ref, hg_ref, qh_ref, ol_ref, state_ref, gg_ref, wl_ref, wa_ref, out_ref
):
    blk = qh_ref.shape[0]
    peers = parts_ref.shape[0]
    lam = lam_ref[0]
    stats = jnp.concatenate(
        [parts_ref[j, blk:, :].astype(F32) for j in range(peers)]
        + [jnp.zeros((LANES - peers * STATS, blk), F32)],
        axis=0,
    ).T
    attended = jnp.zeros((blk, LANES), F32)
    for m in range(2):
        lses = []
        for j in range(peers):
            at = j * STATS + m
            lses.append(
                stats[:, at : at + 1] + stats[:, at + 2 : at + 3] + stats[:, at + 4 : at + 5]
            )
        top = functools.reduce(jnp.maximum, lses)
        shares = [jnp.exp2(v - top) for v in lses]
        whole = functools.reduce(jnp.add, shares)
        mixed = jnp.zeros((blk, LANES), F32)
        for j in range(peers):
            part = parts_ref[j, :blk, m * LANES : (m + 1) * LANES].astype(F32)
            mixed = mixed + part * (shares[j] / whole)
        attended = mixed if m == 0 else attended - lam * mixed
    scale = lax.rsqrt(jnp.mean(attended * attended, -1, keepdims=True) + NORM_EPS)
    attn = (attended * scale * hg_ref[...]).astype(BF16)
    read = dot(qh_ref[...], state_ref[...]) + ol_ref[...]
    centered = read - half_sums(read) * (1.0 / HALF)
    var = half_sums(centered * centered) * (1.0 / HALF)
    linear = centered * lax.rsqrt(var + GROUP_EPS)
    linear = (pltpu.roll(linear, HALF, 1) * gg_ref[...]).astype(BF16)
    width = 512
    for c in range(0, out_ref.shape[1], width):
        out_ref[:, c : c + width] = (
            dot(linear, wl_ref[:, c : c + width]) + dot(attn, wa_ref[:, c : c + width])
        ).astype(BF16)


def swap_cores(x):
    return lax.ppermute(x, "c", [(0, 1), (1, 0)])


def shards(
    tokens,
    norm_gain,
    recept_weight,
    key_weight,
    value_weight,
    decay_down_weight,
    rate_down,
    decay_up,
    rate_up,
    decay_base,
    rate_base,
    decay_extra,
    group_gain,
    attn_query,
    attn_key,
    attn_value,
    query_gain,
    key_gain,
    lambdas,
    head_gain,
    out_linear,
    out_attn,
):
    shape = jax.ShapeDtypeStruct
    depth = tokens.shape[1]
    peers = lax.axis_size("x") * lax.axis_size("c")
    length = tokens.shape[0] * peers
    line = lambda v: v.reshape(1, -1)
    mine = lax.all_gather(tokens, "x")
    other = swap_cores(mine)
    normed, query, key_value = pl.pallas_call(
        qkv_kernel,
        out_shape=(
            shape((length, depth), BF16),
            shape((length, LANES), BF16),
            shape((length, 2 * LANES), BF16),
        ),
        in_specs=[vmem()] * 8,
        out_specs=(vmem(),) * 3,
        compiler_params=params(12),
        cost_estimate=cost(2 * length * depth * 384, 6 << 20),
        name="qkv",
    )(
        mine,
        other,
        line(norm_gain),
        attn_query,
        attn_key,
        attn_value,
        line(jnp.tile(query_gain, 2)),
        line(jnp.tile(key_gain, 2)),
    )
    all_kv = lax.all_gather(key_value, "z", axis=0, tiled=True)
    reader, local_out, payload = pl.pallas_call(
        linear_kernel,
        out_shape=(
            shape((length, LANES), BF16),
            shape((length, LANES), F32),
            shape((length + LANES, LANES), BF16),
        ),
        in_specs=[vmem()] * 12,
        out_specs=(vmem(),) * 3,
        compiler_params=params(20),
        cost_estimate=cost(2 * length * depth * 1024, 6 << 20),
        name="linear",
    )(
        normed,
        query,
        recept_weight,
        key_weight,
        value_weight,
        decay_down_weight.T,
        rate_down.T,
        decay_up,
        rate_up,
        line(decay_base),
        line(rate_base),
        decay_extra.T,
    )
    gathered = lax.all_gather(payload, "y")
    total, before = pl.pallas_call(
        row_kernel,
        out_shape=(shape((LANES, LANES), BF16), shape((LANES, LANES), F32)),
        in_specs=[vmem()],
        out_specs=(vmem(),) * 2,
        compiler_params=params(6),
        cost_estimate=cost(1 << 27, 1 << 20),
        name="row",
    )(gathered)
    totals = lax.all_gather(total, "z")
    state = pl.pallas_call(
        carry_kernel,
        out_shape=shape((LANES, LANES), BF16),
        in_specs=[vmem(), vmem()],
        out_specs=vmem(),
        compiler_params=params(6),
        cost_estimate=cost(1 << 27, 1 << 20),
        name="carry",
    )(totals, before)
    all_kv, state = lax.optimization_barrier((all_kv, state))
    rows_q = gathered.shape[0]
    partial = pl.pallas_call(
        attend_kernel,
        out_shape=shape((rows_q, length + STATS, 2 * LANES), BF16),
        in_specs=[vmem(), pl.BlockSpec(memory_space=pltpu.HBM)],
        out_specs=vmem(),
        scratch_shapes=[
            pltpu.VMEM((2 * rows_q, length, LANES), F32),
            pltpu.VMEM((2 * rows_q, length, 2 * LANES), F32),
            pltpu.VMEM(all_kv.shape, BF16),
            pltpu.VMEM((4 * length, 2 * LANES), BF16),
            pltpu.SemaphoreType.DMA((all_kv.shape[0] // (4 * length),)),
        ],
        compiler_params=params(62),
        cost_estimate=cost(4 * rows_q * length * all_kv.shape[0] * 384, 6 << 20),
        name="attend",
    )(gathered, all_kv)
    parts = lax.all_to_all(partial, "y", split_axis=0, concat_axis=0, tiled=True)
    share = pl.pallas_call(
        finish_kernel,
        out_shape=shape((length, depth), BF16),
        in_specs=[smem()] + [vmem()] * 8,
        out_specs=vmem(),
        compiler_params=params(12),
        cost_estimate=cost(2 * length * depth * 256, 4 << 20),
        name="finish",
    )(
        lambdas,
        parts,
        line(head_gain),
        reader,
        local_out,
        state,
        line(group_gain),
        out_linear,
        out_attn,
    )
    arrived = lax.all_to_all(
        share.reshape(peers, length // peers, depth),
        ("x", "c"),
        split_axis=0,
        concat_axis=0,
        tiled=True,
    )
    return arrived.astype(F32).sum(axis=0).astype(BF16)


def solution(mesh):
    torus = Mesh(mesh.devices.reshape(16, 4, 4, 2), ("z", "y", "x", "c"))
    seq = ("z", "y")
    tp = ("x", "c")
    every = P(seq + tp, None)
    return jax.shard_map(
        shards,
        mesh=torus,
        in_specs=(
            every,
            P(),
            P(None, tp),
            P(None, tp),
            P(None, tp),
            P(),
            P(),
            P(None, tp),
            P(None, tp),
            P(tp),
            P(tp),
            P(seq, tp),
            P(tp),
            P(None, tp),
            P(None, tp),
            P(None, tp),
            P(),
            P(),
            P(tp),
            P(),
            P(tp, None),
            P(tp, None),
        ),
        out_specs=every,
        check_vma=False,
    )
```

```python
import functools

import jax
import jax.numpy as jnp
from jax import lax
from jax.experimental import pallas as pl
from jax.experimental.pallas import tpu as pltpu
from jax.sharding import Mesh
from jax.sharding import PartitionSpec as P

HALF = 64
LANES = 128
F32 = jnp.float32
BF16 = jnp.bfloat16
NORM_EPS = 1e-06
GROUP_EPS = 0.00064
LOG2E = 1.4426950408889634
SCORE = HALF ** (-0.5) * LOG2E
FLOOR = -1e29
MASKED = -1e30
STATS = 16


def vmem():
    return pl.BlockSpec(memory_space=pltpu.VMEM)


def smem():
    return pl.BlockSpec(memory_space=pltpu.SMEM)


def params(mib):
    return pltpu.CompilerParams(vmem_limit_bytes=mib << 20)


def cost(flops, size):
    return pl.CostEstimate(flops=flops, bytes_accessed=size, transcendentals=0)


def low_lanes(shape=(1, LANES)):
    return lax.broadcasted_iota(jnp.int32, shape, len(shape) - 1) < HALF


def half_sums(v):
    low = low_lanes()
    first = jnp.sum(jnp.where(low, v, 0.0), -1, keepdims=True)
    second = jnp.sum(jnp.where(low, 0.0, v), -1, keepdims=True)
    return jnp.where(low, first, second)


def dot(a, b):
    return jnp.dot(a, b, preferred_element_type=F32)


def dot_nt(a, b):
    return lax.dot_general(a, b, (((1,), (1,)), ((), ())), preferred_element_type=F32)


def dot_tn(a, b):
    return lax.dot_general(a, b, (((0,), (0,)), ((), ())), preferred_element_type=F32)


def two_parts(v):
    high = v.astype(BF16)
    return high, (v - high.astype(F32)).astype(BF16)


def dot3(a, b):
    ah, al = two_parts(a)
    bh, bl = two_parts(b)
    return dot(ah, bh) + (dot(ah, bl) + dot(al, bh))


def rounded(v):
    return v.astype(BF16).astype(F32)


def qkv_kernel(
    mine_ref, other_ref, gain_ref, wq_ref, wk_ref, wv_ref, qg_ref, kg_ref, normed_ref, q_ref, kv_ref
):
    core = lax.axis_index("c")
    chips, step, _ = mine_ref.shape

    def turn(i, carry):
        for source, at in ((mine_ref, 2 * i + core), (other_ref, 2 * i + 1 - core)):
            x = source[i].astype(F32)
            scale = lax.rsqrt(jnp.mean(x * x, -1, keepdims=True) + NORM_EPS)
            span = pl.ds(pl.multiple_of(at * step, step), step)
            normed_ref[span, :] = (x * scale * gain_ref[...]).astype(BF16)
        return carry

    lax.fori_loop(0, chips, turn, 0)
    normed = normed_ref[...]

    def map_norm(weight_ref, gain_ref):
        v = rounded(dot(normed, weight_ref[...]))
        scale = lax.rsqrt(half_sums(v * v) * (1.0 / HALF) + NORM_EPS)
        return (v * scale * gain_ref[...]).astype(BF16)

    q_ref[...] = map_norm(wq_ref, qg_ref)
    kv_ref[:, :LANES] = map_norm(wk_ref, kg_ref)
    kv_ref[:, LANES:] = dot(normed, wv_ref[...]).astype(BF16)


def linear_kernel(
    normed_ref,
    q_ref,
    wr_ref,
    wk_ref,
    wv_ref,
    wd_ref,
    wg_ref,
    du_ref,
    ru_ref,
    db_ref,
    rb_ref,
    extra_t_ref,
    qh_ref,
    ol_ref,
    pay_ref,
):
    normed = normed_ref[...]
    length = normed.shape[0]
    low = low_lanes()
    recept = rounded(dot(normed, wr_ref[...]))
    key = rounded(dot(normed, wk_ref[...]))
    value = rounded(dot(normed, wv_ref[...]))
    decay_low = dot_nt(normed, wd_ref[...]).astype(BF16)
    rate_low = dot_nt(normed, wg_ref[...]).astype(BF16)
    log_chan = -jnp.exp(db_ref[...] + jnp.tanh(dot(decay_low, du_ref[...])))
    gate = jax.nn.sigmoid(rb_ref[...] + jnp.tanh(dot(rate_low, ru_ref[...])))
    unit = key * lax.rsqrt(half_sums(key * key) + NORM_EPS)
    head_step = jnp.concatenate(
        [jnp.broadcast_to(extra_t_ref[h : h + 1, :], (HALF, length)) for h in range(2)], axis=0
    ).T
    row = lax.broadcasted_iota(jnp.int32, (length, length), 0)
    col = lax.broadcasted_iota(jnp.int32, (length, length), 1)
    incl = row >= col
    lower = jnp.where(incl, 1.0, 0.0).astype(F32)
    both = jnp.dot(
        lower,
        jnp.concatenate([log_chan, head_step], axis=1),
        preferred_element_type=F32,
        precision=lax.Precision.HIGHEST,
    )
    chan = both[:, :LANES]
    head = both[:, LANES:]
    head_rows = jnp.dot(
        extra_t_ref[...],
        jnp.where(row <= col, 1.0, 0.0).astype(F32),
        preferred_element_type=F32,
        precision=lax.Precision.HIGHEST,
    )
    chan_prev = chan - log_chan
    head_prev = head - head_step
    remove = -unit
    restore = unit * gate
    inject = key * gate
    total = chan + head
    ending = total[length - 1 : length, :]
    to_end = jnp.exp(jnp.minimum(ending - total, 0.0))
    grow = jnp.exp(chan)
    shrink = jnp.exp(-chan)
    left = jnp.concatenate([remove * jnp.exp(chan_prev), recept * grow], axis=0)
    right = jnp.concatenate([restore * shrink, inject * shrink], axis=0).astype(BF16)
    remove_dec = remove * jnp.exp(chan_prev + head_prev)
    recept_dec = recept * jnp.exp(total)
    restore_end = restore * to_end
    inject_end = inject * to_end
    turned = pltpu.roll(value, HALF, 1)
    outs = []
    maps = []
    for h in range(2):
        own = low if h == 0 else jnp.logical_not(low)
        products = dot_nt(jnp.where(own, left, 0.0).astype(BF16), right)
        spread = head[:, h * HALF : h * HALF + 1] - head_rows[h : h + 1, :]
        ratio_incl = jnp.exp(jnp.where(incl, spread, MASKED))
        ratio_strict = jnp.exp(
            jnp.where(row > col, spread - head_step[:, h * HALF : h * HALF + 1], MASKED)
        )
        low_restore = products[:length, :length] * ratio_strict
        low_inject = (products[:length, length:] * ratio_strict).astype(BF16)
        out_restore = (products[length:, :length] * ratio_incl).astype(BF16)
        out_inject = (products[length:, length:] * ratio_incl).astype(BF16)
        inverse = jnp.where(row == col, 1.0, 0.0).astype(F32)
        for level in range((length - 1).bit_length()):
            joint = jnp.right_shift(row, level + 1) == jnp.right_shift(col, level + 1)
            block = joint & (jnp.right_shift(row, level) > jnp.right_shift(col, level))
            part = jnp.where(block, low_restore, 0.0)
            if level == 0:
                inverse = inverse + part
            else:
                known = inverse.astype(BF16)
                inverse = inverse + dot(known, dot(part.astype(BF16), known).astype(BF16))
        other = jnp.where(own, 0.0, turned).astype(BF16)
        sides = jnp.where(own, remove_dec, dot(low_inject, other)).astype(BF16)
        along = dot(inverse.astype(BF16), sides).astype(BF16)
        outs.append(
            dot(out_restore, along) + jnp.where(own, recept_dec, dot(out_inject, other))
        )
        maps.append(
            dot_tn(jnp.where(own, restore_end, 0.0).astype(BF16), along)
            + dot_tn(jnp.where(own, inject_end, 0.0).astype(BF16), other)
        )
    qh_ref[...] = jnp.where(low, outs[0], outs[1]).astype(BF16)
    ol_ref[...] = jnp.where(low, outs[1], outs[0])
    r128 = lax.broadcasted_iota(jnp.int32, (LANES, LANES), 0)
    c128 = lax.broadcasted_iota(jnp.int32, (LANES, LANES), 1)
    pay_ref[:length, :] = q_ref[...]
    pay_ref[length:, :] = (
        maps[0] + maps[1] + jnp.where(r128 == c128, jnp.exp(ending) - 1.0, 0.0)
    ).astype(BF16)


def map_masks():
    r = lax.broadcasted_iota(jnp.int32, (LANES, LANES), 0)
    c = lax.broadcasted_iota(jnp.int32, (LANES, LANES), 1)
    same = (r < HALF) == (c < HALF)
    return same, jnp.where(r == c, 1.0, 0.0).astype(F32)


def compose(later, earlier, same):
    return dot3(jnp.where(same, later, 0.0), earlier) + jnp.where(same, 0.0, later)


def row_kernel(maps_ref, total_ref, before_ref):
    y = lax.axis_index("y")
    same, eye = map_masks()
    peers, rows, _ = maps_ref.shape
    so_far = eye
    before = eye
    for k in range(peers):
        before = jnp.where(y == k, so_far, before)
        one = maps_ref[k, rows - LANES :, :].astype(F32) + eye
        so_far = one if k == 0 else compose(one, so_far, same)
    before_ref[...] = before
    total_ref[...] = (so_far - eye).astype(BF16)


def carry_kernel(totals_ref, before_ref, state_ref):
    z = lax.axis_index("z")
    same, eye = map_masks()
    peers = totals_ref.shape[0]
    level = [
        jnp.where(k < z, totals_ref[k].astype(F32), 0.0) + eye for k in range(peers)
    ]
    while len(level) > 1:
        level = [compose(level[k + 1], level[k], same) for k in range(0, len(level), 2)]
    full = compose(before_ref[...], level[0], same)
    state_ref[...] = jnp.where(same, 0.0, full).astype(BF16)


def attend_kernel(q_ref, kv_hbm, out_ref, top_ref, acc_ref, kv_ref, wide_ref, sems):
    z = lax.axis_index("z")
    y = lax.axis_index("y")
    rows_q = q_ref.shape[0]
    blk = top_ref.shape[1]
    group = 4
    span = group * blk
    low = low_lanes()
    whole = lax.div(z, group)

    def begin(i, carry):
        for part in range(group):
            at = pl.ds(pl.multiple_of(i * span + part * blk, blk), blk)
            pltpu.make_async_copy(kv_hbm.at[at, :], kv_ref.at[at, :], sems.at[i]).start()
        return carry

    begin(whole, 0)
    lax.fori_loop(0, whole, begin, 0)
    wide_ref[:, LANES:] = jnp.ones((span, LANES), BF16)

    def step(index, last):
        at_keys = pl.ds(pl.multiple_of(index * span, span), span)
        pltpu.make_async_copy(
            kv_hbm.at[at_keys, :], kv_ref.at[at_keys, :], sems.at[index]
        ).wait()
        keys = kv_ref[at_keys, :LANES]
        wide_ref[:, :LANES] = kv_ref[at_keys, LANES:]
        wide = wide_ref[...]

        def scores(at):
            own = low if at % 2 == 0 else jnp.logical_not(low)
            q = q_ref[at // 2, :blk, :]
            return dot_nt(jnp.where(own, q, jnp.zeros_like(q)), keys)

        if last:
            row = lax.broadcasted_iota(jnp.int32, (blk, span), 0)
            col = lax.broadcasted_iota(jnp.int32, (blk, span), 1)
            k_place = (jnp.right_shift(col, 8) + index * group) * rows_q + y
            behind = (k_place - z * rows_q) * blk + jnp.bitwise_and(col, blk - 1) - row
        ahead = scores(0)
        for at in range(2 * rows_q):
            s = ahead * SCORE
            if at + 1 < 2 * rows_q:
                ahead = scores(at + 1)
            if last:
                s = jnp.where(behind <= (at // 2) * blk, s, MASKED)
                new = jnp.maximum(jnp.max(s, -1, keepdims=True), FLOOR)
                acc_ref[at] = dot(jnp.exp2(s - new).astype(BF16), wide)
            else:
                old = top_ref[at, :, 0:1]
                new = jnp.maximum(old, jnp.max(s, -1, keepdims=True))
                p = jnp.exp2(s - new).astype(BF16)
                acc_ref[at] = acc_ref[at] * jnp.exp2(old - new) + dot(p, wide)
            top_ref[at] = jnp.broadcast_to(new, (blk, LANES))

    step(whole, True)

    def turn(i, carry):
        step(i, False)
        return carry

    lax.fori_loop(0, whole, turn, 0)
    lane = lax.broadcasted_iota(jnp.int32, (1, LANES), 1)
    for t in range(rows_q):
        stats = jnp.zeros((blk, LANES), F32)
        for m in range(2):
            at = 2 * t + m
            acc = acc_ref[at]
            weight = acc[:, LANES:]
            seen = weight > 0.0
            safe = jnp.where(seen, weight, 1.0)
            out_ref[t, :blk, m * LANES : (m + 1) * LANES] = (acc[:, :LANES] / safe).astype(BF16)
            lse = jnp.where(seen, top_ref[at] + jnp.log2(safe), MASKED)
            high = rounded(lse)
            mid = rounded(lse - high)
            tail = rounded(lse - high - mid)
            stats = jnp.where(lane == m, high, stats)
            stats = jnp.where(lane == 2 + m, mid, stats)
            stats = jnp.where(lane == 4 + m, tail, stats)
        out_ref[t, blk:, :] = stats.T[:STATS, :].astype(BF16)


def finish_kernel(
    lam_ref, parts_ref, hg_ref, qh_ref, ol_ref, state_ref, gg_ref, wl_ref, wa_ref, out_ref
):
    blk = qh_ref.shape[0]
    peers = parts_ref.shape[0]
    lam = lam_ref[0]
    stats = jnp.concatenate(
        [parts_ref[j, blk:, :].astype(F32) for j in range(peers)]
        + [jnp.zeros((LANES - peers * STATS, blk), F32)],
        axis=0,
    ).T
    attended = jnp.zeros((blk, LANES), F32)
    for m in range(2):
        lses = []
        for j in range(peers):
            at = j * STATS + m
            lses.append(
                stats[:, at : at + 1] + stats[:, at + 2 : at + 3] + stats[:, at + 4 : at + 5]
            )
        top = functools.reduce(jnp.maximum, lses)
        shares = [jnp.exp2(v - top) for v in lses]
        whole = functools.reduce(jnp.add, shares)
        mixed = jnp.zeros((blk, LANES), F32)
        for j in range(peers):
            part = parts_ref[j, :blk, m * LANES : (m + 1) * LANES].astype(F32)
            mixed = mixed + part * (shares[j] / whole)
        attended = mixed if m == 0 else attended - lam * mixed
    scale = lax.rsqrt(jnp.mean(attended * attended, -1, keepdims=True) + NORM_EPS)
    attn = (attended * scale * hg_ref[...]).astype(BF16)
    read = dot(qh_ref[...], state_ref[...]) + ol_ref[...]
    centered = read - half_sums(read) * (1.0 / HALF)
    var = half_sums(centered * centered) * (1.0 / HALF)
    linear = centered * lax.rsqrt(var + GROUP_EPS)
    linear = (pltpu.roll(linear, HALF, 1) * gg_ref[...]).astype(BF16)
    width = 512
    for c in range(0, out_ref.shape[1], width):
        out_ref[:, c : c + width] = (
            dot(linear, wl_ref[:, c : c + width]) + dot(attn, wa_ref[:, c : c + width])
        ).astype(BF16)


def swap_cores(x):
    return lax.ppermute(x, "c", [(0, 1), (1, 0)])


def shards(
    tokens,
    norm_gain,
    recept_weight,
    key_weight,
    value_weight,
    decay_down_weight,
    rate_down,
    decay_up,
    rate_up,
    decay_base,
    rate_base,
    decay_extra,
    group_gain,
    attn_query,
    attn_key,
    attn_value,
    query_gain,
    key_gain,
    lambdas,
    head_gain,
    out_linear,
    out_attn,
):
    shape = jax.ShapeDtypeStruct
    depth = tokens.shape[1]
    peers = lax.axis_size("x") * lax.axis_size("c")
    length = tokens.shape[0] * peers
    line = lambda v: v.reshape(1, -1)
    mine = lax.all_gather(tokens, "x")
    other = swap_cores(mine)
    normed, query, key_value = pl.pallas_call(
        qkv_kernel,
        out_shape=(
            shape((length, depth), BF16),
            shape((length, LANES), BF16),
            shape((length, 2 * LANES), BF16),
        ),
        in_specs=[vmem()] * 8,
        out_specs=(vmem(),) * 3,
        compiler_params=params(61),
        cost_estimate=cost(2 * length * depth * 384, 6 << 20),
        name="qkv",
    )(
        mine,
        other,
        line(norm_gain),
        attn_query,
        attn_key,
        attn_value,
        line(jnp.tile(query_gain, 2)),
        line(jnp.tile(key_gain, 2)),
    )
    all_kv = lax.all_gather(key_value, "z", axis=0, tiled=True)
    reader, local_out, payload = pl.pallas_call(
        linear_kernel,
        out_shape=(
            shape((length, LANES), BF16),
            shape((length, LANES), F32),
            shape((length + LANES, LANES), BF16),
        ),
        in_specs=[vmem()] * 12,
        out_specs=(vmem(),) * 3,
        compiler_params=params(20),
        cost_estimate=cost(2 * length * depth * 1024, 6 << 20),
        name="linear",
    )(
        normed,
        query,
        recept_weight,
        key_weight,
        value_weight,
        decay_down_weight.T,
        rate_down.T,
        decay_up,
        rate_up,
        line(decay_base),
        line(rate_base),
        decay_extra.T,
    )
    gathered = lax.all_gather(payload, "y")
    total, before = pl.pallas_call(
        row_kernel,
        out_shape=(shape((LANES, LANES), BF16), shape((LANES, LANES), F32)),
        in_specs=[vmem()],
        out_specs=(vmem(),) * 2,
        compiler_params=params(6),
        cost_estimate=cost(1 << 27, 1 << 20),
        name="row",
    )(gathered)
    totals = lax.all_gather(total, "z")
    state = pl.pallas_call(
        carry_kernel,
        out_shape=shape((LANES, LANES), BF16),
        in_specs=[vmem(), vmem()],
        out_specs=vmem(),
        compiler_params=params(6),
        cost_estimate=cost(1 << 27, 1 << 20),
        name="carry",
    )(totals, before)
    all_kv, state = lax.optimization_barrier((all_kv, state))
    rows_q = gathered.shape[0]
    partial = pl.pallas_call(
        attend_kernel,
        out_shape=shape((rows_q, length + STATS, 2 * LANES), BF16),
        in_specs=[vmem(), pl.BlockSpec(memory_space=pltpu.HBM)],
        out_specs=vmem(),
        scratch_shapes=[
            pltpu.VMEM((2 * rows_q, length, LANES), F32),
            pltpu.VMEM((2 * rows_q, length, 2 * LANES), F32),
            pltpu.VMEM(all_kv.shape, BF16),
            pltpu.VMEM((4 * length, 2 * LANES), BF16),
            pltpu.SemaphoreType.DMA((all_kv.shape[0] // (4 * length),)),
        ],
        compiler_params=params(62),
        cost_estimate=cost(4 * rows_q * length * all_kv.shape[0] * 384, 6 << 20),
        name="attend",
    )(gathered, all_kv)
    parts = lax.all_to_all(partial, "y", split_axis=0, concat_axis=0, tiled=True)
    share = pl.pallas_call(
        finish_kernel,
        out_shape=shape((length, depth), BF16),
        in_specs=[smem()] + [vmem()] * 8,
        out_specs=vmem(),
        compiler_params=params(12),
        cost_estimate=cost(2 * length * depth * 256, 4 << 20),
        name="finish",
    )(
        lambdas,
        parts,
        line(head_gain),
        reader,
        local_out,
        state,
        line(group_gain),
        out_linear,
        out_attn,
    )
    arrived = lax.all_to_all(
        share.reshape(peers, length // peers, depth),
        ("x", "c"),
        split_axis=0,
        concat_axis=0,
        tiled=True,
    )
    return arrived.astype(F32).sum(axis=0).astype(BF16)


def solution(mesh):
    torus = Mesh(mesh.devices.reshape(16, 4, 4, 2), ("z", "y", "x", "c"))
    seq = ("z", "y")
    tp = ("x", "c")
    every = P(seq + tp, None)
    return jax.shard_map(
        shards,
        mesh=torus,
        in_specs=(
            every,
            P(),
            P(None, tp),
            P(None, tp),
            P(None, tp),
            P(),
            P(),
            P(None, tp),
            P(None, tp),
            P(tp),
            P(tp),
            P(seq, tp),
            P(tp),
            P(None, tp),
            P(None, tp),
            P(None, tp),
            P(),
            P(),
            P(tp),
            P(),
            P(tp, None),
            P(tp, None),
        ),
        out_specs=every,
        check_vma=False,
    )
```

```python
import functools

import jax
import jax.numpy as jnp
from jax import lax
from jax.experimental import pallas as pl
from jax.experimental.pallas import tpu as pltpu
from jax.sharding import Mesh
from jax.sharding import PartitionSpec as P

HALF = 64
LANES = 128
F32 = jnp.float32
BF16 = jnp.bfloat16
NORM_EPS = 1e-06
GROUP_EPS = 0.00064
LOG2E = 1.4426950408889634
SCORE = HALF ** (-0.5) * LOG2E
FLOOR = -1e29
MASKED = -1e30
STATS = 16


def vmem():
    return pl.BlockSpec(memory_space=pltpu.VMEM)


def smem():
    return pl.BlockSpec(memory_space=pltpu.SMEM)


def params(mib):
    return pltpu.CompilerParams(vmem_limit_bytes=mib << 20)


def cost(flops, size):
    return pl.CostEstimate(flops=flops, bytes_accessed=size, transcendentals=0)


def low_lanes(shape=(1, LANES)):
    return lax.broadcasted_iota(jnp.int32, shape, len(shape) - 1) < HALF


def half_sums(v):
    low = low_lanes()
    first = jnp.sum(jnp.where(low, v, 0.0), -1, keepdims=True)
    second = jnp.sum(jnp.where(low, 0.0, v), -1, keepdims=True)
    return jnp.where(low, first, second)


def dot(a, b):
    return jnp.dot(a, b, preferred_element_type=F32)


def dot_nt(a, b):
    return lax.dot_general(a, b, (((1,), (1,)), ((), ())), preferred_element_type=F32)


def dot_tn(a, b):
    return lax.dot_general(a, b, (((0,), (0,)), ((), ())), preferred_element_type=F32)


def two_parts(v):
    high = v.astype(BF16)
    return high, (v - high.astype(F32)).astype(BF16)


def dot3(a, b):
    ah, al = two_parts(a)
    bh, bl = two_parts(b)
    return dot(ah, bh) + (dot(ah, bl) + dot(al, bh))


def rounded(v):
    return v.astype(BF16).astype(F32)


def qkv_kernel(
    mine_ref, other_ref, gain_ref, wq_ref, wk_ref, wv_ref, qg_ref, kg_ref, normed_ref, q_ref, kv_ref
):
    core = lax.axis_index("c")
    chips, step, _ = mine_ref.shape

    def turn(i, carry):
        for source, at in ((mine_ref, 2 * i + core), (other_ref, 2 * i + 1 - core)):
            x = source[i].astype(F32)
            scale = lax.rsqrt(jnp.mean(x * x, -1, keepdims=True) + NORM_EPS)
            span = pl.ds(pl.multiple_of(at * step, step), step)
            normed_ref[span, :] = (x * scale * gain_ref[...]).astype(BF16)
        return carry

    lax.fori_loop(0, chips, turn, 0)
    normed = normed_ref[...]

    def map_norm(weight_ref, gain_ref):
        v = rounded(dot(normed, weight_ref[...]))
        scale = lax.rsqrt(half_sums(v * v) * (1.0 / HALF) + NORM_EPS)
        return (v * scale * gain_ref[...]).astype(BF16)

    q_ref[...] = map_norm(wq_ref, qg_ref)
    kv_ref[:, :LANES] = map_norm(wk_ref, kg_ref)
    kv_ref[:, LANES:] = dot(normed, wv_ref[...]).astype(BF16)


def linear_kernel(
    normed_ref,
    q_ref,
    wr_ref,
    wk_ref,
    wv_ref,
    wd_ref,
    wg_ref,
    du_ref,
    ru_ref,
    db_ref,
    rb_ref,
    extra_t_ref,
    qh_ref,
    ol_ref,
    pay_ref,
):
    normed = normed_ref[...]
    length = normed.shape[0]
    low = low_lanes()
    recept = rounded(dot(normed, wr_ref[...]))
    key = rounded(dot(normed, wk_ref[...]))
    value = rounded(dot(normed, wv_ref[...]))
    decay_low = dot_nt(normed, wd_ref[...]).astype(BF16)
    rate_low = dot_nt(normed, wg_ref[...]).astype(BF16)
    log_chan = -jnp.exp(db_ref[...] + jnp.tanh(dot(decay_low, du_ref[...])))
    gate = jax.nn.sigmoid(rb_ref[...] + jnp.tanh(dot(rate_low, ru_ref[...])))
    unit = key * lax.rsqrt(half_sums(key * key) + NORM_EPS)
    head_step = jnp.concatenate(
        [jnp.broadcast_to(extra_t_ref[h : h + 1, :], (HALF, length)) for h in range(2)], axis=0
    ).T
    row = lax.broadcasted_iota(jnp.int32, (length, length), 0)
    col = lax.broadcasted_iota(jnp.int32, (length, length), 1)
    incl = row >= col
    lower = jnp.where(incl, 1.0, 0.0).astype(F32)
    both = jnp.dot(
        lower,
        jnp.concatenate([log_chan, head_step], axis=1),
        preferred_element_type=F32,
        precision=lax.Precision.HIGHEST,
    )
    chan = both[:, :LANES]
    head = both[:, LANES:]
    head_rows = jnp.dot(
        extra_t_ref[...],
        jnp.where(row <= col, 1.0, 0.0).astype(F32),
        preferred_element_type=F32,
        precision=lax.Precision.HIGHEST,
    )
    chan_prev = chan - log_chan
    head_prev = head - head_step
    remove = -unit
    restore = unit * gate
    inject = key * gate
    total = chan + head
    ending = total[length - 1 : length, :]
    to_end = jnp.exp(jnp.minimum(ending - total, 0.0))
    grow = jnp.exp(chan)
    shrink = jnp.exp(-chan)
    left = jnp.concatenate([remove * jnp.exp(chan_prev), recept * grow], axis=0)
    right = jnp.concatenate([restore * shrink, inject * shrink], axis=0).astype(BF16)
    remove_dec = remove * jnp.exp(chan_prev + head_prev)
    recept_dec = recept * jnp.exp(total)
    restore_end = restore * to_end
    inject_end = inject * to_end
    turned = pltpu.roll(value, HALF, 1)
    outs = []
    maps = []
    for h in range(2):
        own = low if h == 0 else jnp.logical_not(low)
        products = dot_nt(jnp.where(own, left, 0.0).astype(BF16), right)
        spread = head[:, h * HALF : h * HALF + 1] - head_rows[h : h + 1, :]
        ratio_incl = jnp.exp(jnp.where(incl, spread, MASKED))
        ratio_strict = jnp.exp(
            jnp.where(row > col, spread - head_step[:, h * HALF : h * HALF + 1], MASKED)
        )
        low_restore = products[:length, :length] * ratio_strict
        low_inject = (products[:length, length:] * ratio_strict).astype(BF16)
        out_restore = (products[length:, :length] * ratio_incl).astype(BF16)
        out_inject = (products[length:, length:] * ratio_incl).astype(BF16)
        inverse = jnp.where(row == col, 1.0, 0.0).astype(F32)
        for level in range((length - 1).bit_length()):
            joint = jnp.right_shift(row, level + 1) == jnp.right_shift(col, level + 1)
            block = joint & (jnp.right_shift(row, level) > jnp.right_shift(col, level))
            part = jnp.where(block, low_restore, 0.0)
            if level == 0:
                inverse = inverse + part
            else:
                known = inverse.astype(BF16)
                inverse = inverse + dot(known, dot(part.astype(BF16), known).astype(BF16))
        other = jnp.where(own, 0.0, turned).astype(BF16)
        sides = jnp.where(own, remove_dec, dot(low_inject, other)).astype(BF16)
        along = dot(inverse.astype(BF16), sides).astype(BF16)
        outs.append(
            dot(out_restore, along) + jnp.where(own, recept_dec, dot(out_inject, other))
        )
        maps.append(
            dot_tn(jnp.where(own, restore_end, 0.0).astype(BF16), along)
            + dot_tn(jnp.where(own, inject_end, 0.0).astype(BF16), other)
        )
    qh_ref[...] = jnp.where(low, outs[0], outs[1]).astype(BF16)
    ol_ref[...] = jnp.where(low, outs[1], outs[0])
    r128 = lax.broadcasted_iota(jnp.int32, (LANES, LANES), 0)
    c128 = lax.broadcasted_iota(jnp.int32, (LANES, LANES), 1)
    pay_ref[:length, :] = q_ref[...]
    pay_ref[length:, :] = (
        maps[0] + maps[1] + jnp.where(r128 == c128, jnp.exp(ending) - 1.0, 0.0)
    ).astype(BF16)


def map_masks():
    r = lax.broadcasted_iota(jnp.int32, (LANES, LANES), 0)
    c = lax.broadcasted_iota(jnp.int32, (LANES, LANES), 1)
    same = (r < HALF) == (c < HALF)
    return same, jnp.where(r == c, 1.0, 0.0).astype(F32)


def compose(later, earlier, same):
    return dot3(jnp.where(same, later, 0.0), earlier) + jnp.where(same, 0.0, later)


def row_kernel(maps_ref, total_ref, before_ref):
    y = lax.axis_index("zl") * lax.axis_size("y") + lax.axis_index("y")
    same, eye = map_masks()
    peers, rows, _ = maps_ref.shape
    so_far = eye
    before = eye
    for k in range(peers):
        before = jnp.where(y == k, so_far, before)
        one = maps_ref[k, rows - LANES :, :].astype(F32) + eye
        so_far = one if k == 0 else compose(one, so_far, same)
    before_ref[...] = before
    total_ref[...] = (so_far - eye).astype(BF16)


def carry_kernel(totals_ref, before_ref, state_ref):
    z = lax.axis_index("zp")
    same, eye = map_masks()
    peers = totals_ref.shape[0]
    level = [
        jnp.where(k < z, totals_ref[k].astype(F32), 0.0) + eye for k in range(peers)
    ]
    while len(level) > 1:
        level = [compose(level[k + 1], level[k], same) for k in range(0, len(level), 2)]
    full = compose(before_ref[...], level[0], same)
    state_ref[...] = jnp.where(same, 0.0, full).astype(BF16)


def attend_kernel(q_ref, kv_hbm, out_ref, top_ref, acc_ref, kv_ref, wide_ref, sems):
    z = lax.axis_index("zp")
    y = lax.axis_index("zl") * lax.axis_size("y") + lax.axis_index("y")
    rows_q = q_ref.shape[0]
    blk = top_ref.shape[1]
    group = 4
    span = group * blk
    low = low_lanes()
    whole = lax.div(z, group)

    def begin(i, carry):
        for part in range(group):
            at = pl.ds(pl.multiple_of(i * span + part * blk, blk), blk)
            pltpu.make_async_copy(kv_hbm.at[at, :], kv_ref.at[at, :], sems.at[i]).start()
        return carry

    begin(whole, 0)
    lax.fori_loop(0, whole, begin, 0)
    wide_ref[:, LANES:] = jnp.ones((span, LANES), BF16)

    def step(index, last):
        at_keys = pl.ds(pl.multiple_of(index * span, span), span)
        pltpu.make_async_copy(
            kv_hbm.at[at_keys, :], kv_ref.at[at_keys, :], sems.at[index]
        ).wait()
        keys = kv_ref[at_keys, :LANES]
        wide_ref[:, :LANES] = kv_ref[at_keys, LANES:]
        wide = wide_ref[...]

        def scores(at):
            own = low if at % 2 == 0 else jnp.logical_not(low)
            q = q_ref[at // 2, :blk, :]
            return dot_nt(jnp.where(own, q, jnp.zeros_like(q)), keys)

        if last:
            row = lax.broadcasted_iota(jnp.int32, (blk, span), 0)
            col = lax.broadcasted_iota(jnp.int32, (blk, span), 1)
            k_place = (jnp.right_shift(col, 8) + index * group) * rows_q + y
            behind = (k_place - z * rows_q) * blk + jnp.bitwise_and(col, blk - 1) - row
        ahead = scores(0)
        for at in range(2 * rows_q):
            s = ahead * SCORE
            if at + 1 < 2 * rows_q:
                ahead = scores(at + 1)
            if last:
                s = jnp.where(behind <= (at // 2) * blk, s, MASKED)
                new = jnp.maximum(jnp.max(s, -1, keepdims=True), FLOOR)
                acc_ref[at] = dot(jnp.exp2(s - new).astype(BF16), wide)
            else:
                old = top_ref[at, :, 0:1]
                new = jnp.maximum(old, jnp.max(s, -1, keepdims=True))
                p = jnp.exp2(s - new).astype(BF16)
                acc_ref[at] = acc_ref[at] * jnp.exp2(old - new) + dot(p, wide)
            top_ref[at] = jnp.broadcast_to(new, (blk, LANES))

    step(whole, True)

    def turn(i, carry):
        step(i, False)
        return carry

    lax.fori_loop(0, whole, turn, 0)
    lane = lax.broadcasted_iota(jnp.int32, (1, LANES), 1)
    for t in range(rows_q):
        stats = jnp.zeros((blk, LANES), F32)
        for m in range(2):
            at = 2 * t + m
            acc = acc_ref[at]
            weight = acc[:, LANES:]
            seen = weight > 0.0
            safe = jnp.where(seen, weight, 1.0)
            out_ref[t, :blk, m * LANES : (m + 1) * LANES] = (acc[:, :LANES] / safe).astype(BF16)
            lse = jnp.where(seen, top_ref[at] + jnp.log2(safe), MASKED)
            high = rounded(lse)
            mid = rounded(lse - high)
            tail = rounded(lse - high - mid)
            stats = jnp.where(lane == m, high, stats)
            stats = jnp.where(lane == 2 + m, mid, stats)
            stats = jnp.where(lane == 4 + m, tail, stats)
        out_ref[t, blk:, :] = stats.T[:STATS, :].astype(BF16)


def finish_kernel(
    lam_ref, parts_ref, hg_ref, qh_ref, ol_ref, state_ref, gg_ref, wl_ref, wa_ref, out_ref
):
    blk = qh_ref.shape[0]
    peers = parts_ref.shape[0]
    lam = lam_ref[0]
    stats = jnp.concatenate(
        [parts_ref[j, blk:, :].astype(F32) for j in range(peers)], axis=0
    ).T
    attended = jnp.zeros((blk, LANES), F32)
    for m in range(2):
        lses = []
        for j in range(peers):
            at = j * STATS + m
            lses.append(
                stats[:, at : at + 1] + stats[:, at + 2 : at + 3] + stats[:, at + 4 : at + 5]
            )
        top = functools.reduce(jnp.maximum, lses)
        shares = [jnp.exp2(v - top) for v in lses]
        whole = functools.reduce(jnp.add, shares)
        mixed = jnp.zeros((blk, LANES), F32)
        for j in range(peers):
            part = parts_ref[j, :blk, m * LANES : (m + 1) * LANES].astype(F32)
            mixed = mixed + part * (shares[j] / whole)
        attended = mixed if m == 0 else attended - lam * mixed
    scale = lax.rsqrt(jnp.mean(attended * attended, -1, keepdims=True) + NORM_EPS)
    attn = (attended * scale * hg_ref[...]).astype(BF16)
    read = dot(qh_ref[...], state_ref[...]) + ol_ref[...]
    centered = read - half_sums(read) * (1.0 / HALF)
    var = half_sums(centered * centered) * (1.0 / HALF)
    linear = centered * lax.rsqrt(var + GROUP_EPS)
    linear = (pltpu.roll(linear, HALF, 1) * gg_ref[...]).astype(BF16)
    width = 512
    for c in range(0, out_ref.shape[1], width):
        out_ref[:, c : c + width] = (
            dot(linear, wl_ref[:, c : c + width]) + dot(attn, wa_ref[:, c : c + width])
        ).astype(BF16)


def copy_for_each(x, axes):
    copies = jnp.broadcast_to(x, (lax.axis_size(axes), *x.shape))
    return lax.all_to_all(copies, axes, split_axis=0, concat_axis=0, tiled=True)


def swap_cores(x):
    return lax.ppermute(x, "c", [(0, 1), (1, 0)])


def shards(
    tokens,
    norm_gain,
    recept_weight,
    key_weight,
    value_weight,
    decay_down_weight,
    rate_down,
    decay_up,
    rate_up,
    decay_base,
    rate_base,
    decay_extra,
    group_gain,
    attn_query,
    attn_key,
    attn_value,
    query_gain,
    key_gain,
    lambdas,
    head_gain,
    out_linear,
    out_attn,
):
    shape = jax.ShapeDtypeStruct
    depth = tokens.shape[1]
    peers = lax.axis_size("x") * lax.axis_size("c")
    length = tokens.shape[0] * peers
    line = lambda v: v.reshape(1, -1)
    mine = lax.all_gather(tokens, "x")
    other = swap_cores(mine)
    normed, query, key_value = pl.pallas_call(
        qkv_kernel,
        out_shape=(
            shape((length, depth), BF16),
            shape((length, LANES), BF16),
            shape((length, 2 * LANES), BF16),
        ),
        in_specs=[vmem()] * 8,
        out_specs=(vmem(),) * 3,
        compiler_params=params(61),
        cost_estimate=cost(2 * length * depth * 384, 6 << 20),
        name="qkv",
    )(
        mine,
        other,
        line(norm_gain),
        attn_query,
        attn_key,
        attn_value,
        line(jnp.tile(query_gain, 2)),
        line(jnp.tile(key_gain, 2)),
    )
    all_kv = lax.all_gather(key_value, "zp", axis=0, tiled=True)
    reader, local_out, payload = pl.pallas_call(
        linear_kernel,
        out_shape=(
            shape((length, LANES), BF16),
            shape((length, LANES), F32),
            shape((length + LANES, LANES), BF16),
        ),
        in_specs=[vmem()] * 12,
        out_specs=(vmem(),) * 3,
        compiler_params=params(20),
        cost_estimate=cost(2 * length * depth * 1024, 6 << 20),
        name="linear",
    )(
        normed,
        query,
        recept_weight,
        key_weight,
        value_weight,
        decay_down_weight.T,
        rate_down.T,
        decay_up,
        rate_up,
        line(decay_base),
        line(rate_base),
        decay_extra.T,
    )
    gathered = copy_for_each(payload, ("zl", "y"))
    total, before = pl.pallas_call(
        row_kernel,
        out_shape=(shape((LANES, LANES), BF16), shape((LANES, LANES), F32)),
        in_specs=[vmem()],
        out_specs=(vmem(),) * 2,
        compiler_params=params(6),
        cost_estimate=cost(1 << 27, 1 << 20),
        name="row",
    )(gathered)
    totals = copy_for_each(total, "zp")
    state = pl.pallas_call(
        carry_kernel,
        out_shape=shape((LANES, LANES), BF16),
        in_specs=[vmem(), vmem()],
        out_specs=vmem(),
        compiler_params=params(6),
        cost_estimate=cost(1 << 27, 1 << 20),
        name="carry",
    )(totals, before)
    all_kv, state = lax.optimization_barrier((all_kv, state))
    rows_q = gathered.shape[0]
    partial = pl.pallas_call(
        attend_kernel,
        out_shape=shape((rows_q, length + STATS, 2 * LANES), BF16),
        in_specs=[vmem(), pl.BlockSpec(memory_space=pltpu.HBM)],
        out_specs=vmem(),
        scratch_shapes=[
            pltpu.VMEM((2 * rows_q, length, LANES), F32),
            pltpu.VMEM((2 * rows_q, length, 2 * LANES), F32),
            pltpu.VMEM(all_kv.shape, BF16),
            pltpu.VMEM((4 * length, 2 * LANES), BF16),
            pltpu.SemaphoreType.DMA((all_kv.shape[0] // (4 * length),)),
        ],
        compiler_params=params(62),
        cost_estimate=cost(4 * rows_q * length * all_kv.shape[0] * 384, 6 << 20),
        name="attend",
    )(gathered, all_kv)
    parts = lax.all_to_all(partial, ("zl", "y"), split_axis=0, concat_axis=0, tiled=True)
    share = pl.pallas_call(
        finish_kernel,
        out_shape=shape((length, depth), BF16),
        in_specs=[smem()] + [vmem()] * 8,
        out_specs=vmem(),
        compiler_params=params(12),
        cost_estimate=cost(2 * length * depth * 256, 4 << 20),
        name="finish",
    )(
        lambdas,
        parts,
        line(head_gain),
        reader,
        local_out,
        state,
        line(group_gain),
        out_linear,
        out_attn,
    )
    arrived = lax.all_to_all(
        share.reshape(peers, length // peers, depth),
        ("x", "c"),
        split_axis=0,
        concat_axis=0,
        tiled=True,
    )
    return arrived.astype(F32).sum(axis=0).astype(BF16)


def solution(mesh):
    torus = Mesh(mesh.devices.reshape(8, 2, 4, 4, 2), ("zp", "zl", "y", "x", "c"))
    seq = ("zp", "zl", "y")
    tp = ("x", "c")
    every = P(seq + tp, None)
    return jax.shard_map(
        shards,
        mesh=torus,
        in_specs=(
            every,
            P(),
            P(None, tp),
            P(None, tp),
            P(None, tp),
            P(),
            P(),
            P(None, tp),
            P(None, tp),
            P(tp),
            P(tp),
            P(seq, tp),
            P(tp),
            P(None, tp),
            P(None, tp),
            P(None, tp),
            P(),
            P(),
            P(tp),
            P(),
            P(tp, None),
            P(tp, None),
        ),
        out_specs=every,
        check_vma=False,
    )
```
